128 devices in a mesh: fs: 32 (over z, y, core), tp: 4 (over x).
Axes of the slice: x: 4, y: 4, z: 4, core: 2. Of those that a mesh axis runs over, the one named last changes fastest.
Arguments:
- model_input: bfloat16 [65536, 2048], P('fs'), may hold values from -6 to 6
- value_cotan: bfloat16 [65536, 2048], P('fs', 'tp'), may hold values from -0.0234375 to 0.0234375
- mixer_cotan: bfloat16 [65536, 2048], P('fs'), may hold values from -0.0234375 to 0.0234375
- head_output: bfloat16 [65536, 2048], P('fs', 'tp'), may hold values from -6 to 6
- value_weight: float32 [2048, 2048], P('fs', 'tp'), may hold values from -0.125 to 0.125
- value_factor: bfloat16 [2048, 512], P('fs'), may hold values from -0.125 to 0.125
- value_first: float32 [512, 2048], P('fs', 'tp'), may hold values from -3 to 3
- value_second: float32 [512, 2048], P('fs', 'tp'), may hold values from 0.02 to 0.5
- output_weight: float32 [2048, 2048], P('fs', 'tp'), may hold values from -0.125 to 0.125
- output_factor: bfloat16 [2048, 512], P('fs'), may hold values from -0.125 to 0.125
- output_first: float32 [512, 2048], P('fs', 'tp'), may hold values from -3 to 3
- output_second: float32 [512, 2048], P('fs', 'tp'), may hold values from 0.02 to 0.5
Outputs:
- value_step: float32 [2048, 2048], P('fs', 'tp')
- value_updated: float32 [2048, 2048], P('fs', 'tp')
- value_first_new: float32 [512, 2048], P('fs', 'tp')
- value_second_new: float32 [512, 2048], P('fs', 'tp')
- value_copy: bfloat16 [2048, 2048], P(None, 'tp')
- output_step: float32 [2048, 2048], P('fs', 'tp')
- output_updated: float32 [2048, 2048], P('fs', 'tp')
- output_first_new: float32 [512, 2048], P('fs', 'tp')
- output_second_new: float32 [512, 2048], P('fs', 'tp')
- output_copy: bfloat16 [2048, 2048], P(None, 'tp')
The draws below stay inside these ranges and needn't reach their ends.
All inputs are finite; a program needn't handle non-finite values.
Results may differ from the reference program's by a relative error of at most 0.0059.
Values may be sent and summed in bfloat16 or wider, within the bound.
A program may use at most 128 MiB of HBM per device.

```python
import math
import jax
import jax.numpy as jnp
from jax import lax

D = 2048
RANK = 512
TOK_DEV = 2048
HV = 2048
TOKENS = 65536
N_FS = 32


def with_spikes(array, stream_key, source, target, blocks, factor):
    def block_of(dim):
        return (jnp.arange(array.shape[dim]) // (array.shape[dim] // blocks)).reshape((-1,) + (1,) * (array.ndim - 1 - dim))

    near = jax.random.permutation(stream_key, blocks)[block_of(target)]
    second = (block_of(target) + blocks // 2) % blocks
    return jnp.where((block_of(source) == near) | (block_of(source) == second), factor * array, array)


def steps_of(stream_key, extent, shards, low, high):
    level, own = 1.0, jax.random.fold_in(stream_key, 6)
    for position, shards_of in shards:
        steps = jnp.exp(jax.random.uniform(jax.random.fold_in(own, position), (shards_of,), jnp.float32, low / len(shards), high / len(shards)))
        level = level * jnp.repeat(steps, extent[position] // shards_of).reshape([-1 if axis == position else 1 for axis in range(len(extent))])
    return level


def bell_draw(own_key, extent, spread, limit, shards=(), dtype=jnp.bfloat16):
    array = jax.random.normal(own_key, extent, jnp.float32) * spread
    if len(shards) > 0:
        array = steps_of(own_key, extent, shards, -0.22, 0.18) * array
    return jnp.clip(array, min=-limit, max=limit).astype(dtype)


def noise_with(own_key, extent, spread, bound, cuts, heavy, kind=jnp.bfloat16):
    result = spread * jax.random.normal(own_key, extent, jnp.float32)
    if cuts:
        result = result * steps_of(own_key, extent, cuts, -0.22, 0.18)
    return jnp.clip(with_spikes(result, jax.random.fold_in(own_key, 3), *heavy), -bound, bound).astype(kind)


def setup_inputs(seed: int = 0) -> dict:
    arg_keys = jax.random.split(jax.random.key(seed), 13)
    model_input = noise_with(arg_keys[0], (TOKENS, D), 1.0, 6.0, ((0, 32),), (0, 1, 32, 2.75))
    value_cotan = bell_draw(arg_keys[1], (TOKENS, HV), ((TOK_DEV * N_FS) ** -0.5), 0.0234375, ((0, 32), (1, 4)))
    mixer_cotan = noise_with(arg_keys[2], (TOKENS, D), ((TOK_DEV * N_FS) ** -0.5), 0.0234375, ((0, 32),), (0, 1, 32, 2.75))
    head_output = bell_draw(arg_keys[3], (TOKENS, HV), 1.0, 6.0, ((0, 32), (1, 4)))
    value_weight = bell_draw(arg_keys[4], (D, HV), D ** -0.5, 0.125, ((0, 32), (1, 4)), jnp.float32)
    value_factor = bell_draw(arg_keys[5], (D, RANK), D ** -0.5, 0.125, ((0, 32),))
    value_first = bell_draw(arg_keys[6], (RANK, HV), 0.5, 3.0, ((0, 32), (1, 4)), jnp.float32)
    value_second = jnp.clip(jnp.exp(math.log(0.5) - 3.218876 * jax.random.uniform(arg_keys[7], (RANK, HV), jnp.float32) ** steps_of(arg_keys[7], (RANK, HV), ((0, 32), (1, 4)), -0.2, 0.2)), 0.02, 0.5)
    output_weight = bell_draw(arg_keys[8], (D, HV), HV ** -0.5, 0.125, ((0, 32), (1, 4)), jnp.float32)
    output_factor = bell_draw(arg_keys[9], (D, RANK), D ** -0.5, 0.125, ((0, 32),))
    output_first = bell_draw(arg_keys[10], (RANK, HV), 0.5, 3.0, ((0, 32), (1, 4)), jnp.float32)
    output_second = jnp.clip(jnp.exp(math.log(0.5) - 3.218876 * jax.random.uniform(arg_keys[11], (RANK, HV), jnp.float32) ** steps_of(arg_keys[11], (RANK, HV), ((0, 32), (1, 4)), -0.2, 0.2)), 0.02, 0.5)
    return dict(model_input=model_input, value_cotan=value_cotan, mixer_cotan=mixer_cotan, head_output=head_output, value_weight=value_weight, value_factor=value_factor, value_first=value_first, value_second=value_second, output_weight=output_weight, output_factor=output_factor, output_first=output_first, output_second=output_second)


beta_first = 0.8
beta_second = 0.9
step_rate = 0.02
scale_floor = 0.25
tiny_eps = 1e-08

def low_rank(rows_in, cols_in, factor, first_moment, second_moment):
    gradient = jnp.dot(rows_in.T, cols_in, preferred_element_type=jnp.float32)
    projected = jnp.dot(factor.astype(jnp.float32).T, gradient, precision=lax.Precision.HIGHEST)
    first_new = beta_first * first_moment + (1.0 - beta_first) * projected
    second_new = beta_second * second_moment + (1.0 - beta_second) * projected * projected
    direction = (first_new / (jnp.sqrt(second_new) + tiny_eps)).astype(jnp.bfloat16)
    expanded = jnp.dot(factor, direction, preferred_element_type=jnp.float32)
    return (expanded, first_new, second_new)

def finish(expanded, weight):
    mean_square = jnp.sum(expanded * expanded) / (D * HV)
    update_step = step_rate / jnp.sqrt(mean_square + scale_floor) * expanded
    updated = weight - update_step
    return (update_step, updated, updated.astype(jnp.bfloat16))

def reference(model_input, value_cotan, mixer_cotan, head_output, value_weight, value_factor, value_first, value_second, output_weight, output_factor, output_first, output_second):
    value_exp, value_fnew, value_snew = low_rank(model_input, value_cotan, value_factor, value_first, value_second)
    output_exp, output_fnew, output_snew = low_rank(mixer_cotan, head_output, output_factor, output_first, output_second)
    value_step, value_updated, value_copy = finish(value_exp, value_weight)
    output_step, output_updated, output_copy = finish(output_exp, output_weight)
    return (value_step, value_updated, value_fnew, value_snew, value_copy, output_step, output_updated, output_fnew, output_snew, output_copy)
```

```python
import functools

import jax
import jax.numpy as jnp
from jax import lax
from jax.experimental import pallas as pl
from jax.experimental.pallas import tpu as pltpu
from jax.sharding import PartitionSpec as P

beta_first = 0.8
beta_second = 0.9
step_rate = 0.02
scale_floor = 0.25
tiny_eps = 1e-08

MESH = pl.DeviceIdType.MESH
F32 = jnp.float32
BF16 = jnp.bfloat16
NZ = 4
NC = 2
NQ = 4
WS = 4
GN = 256
N_SEMS = 240
OFFSETS = sorted(
    [(a, b) for a in range(NZ) for b in range(NZ) if a or b],
    key=lambda o: -(min(o[0], NZ - o[0]) + min(o[1], NZ - o[1])),
)


def gather_kernel(
    ntp,
    rows_v, cols_v, rows_o, cols_o,
    fac_v, fac_o, w_v, w_o, first_v, first_o, second_v, second_o,
    fnew_v, snew_v, fnew_o, snew_o, ss_out, fg_out, wg_out, dir_out,
    rows, cols, cols_t, grad, fg, wg, pf, send_a, recv_a, send_b, recv_b, pg,
    dirg, gram, ss, ssg,
    sem_rows, sem_cols, sem_out, ssem, rsem,
):
    me = lax.axis_index("fs")
    tp = lax.axis_index("tp")
    z, y, c = me // (NZ * NC), lax.rem(me // NC, NZ), lax.rem(me, NC)
    co = 1 - c
    chip = z * NZ + y
    h = lax.rem(tp, 2)
    T, D = rows_v.shape
    C = cols_v.shape[1]
    R = fac_v.shape[1]
    QR = fac_v.shape[0] // NQ
    WR = w_v.shape[0] // WS

    def up(a, d):
        return lax.rem(a + d, NZ)

    def dn(a, d):
        return lax.rem(a + NZ - d, NZ)

    def plane(zz, yy):
        return ((zz * NZ + yy) * NC + c, tp)

    mate = (me - c + co, tp)

    def along_x(d):
        return (me, lax.rem(tp + ntp + d, ntp))

    n_used = [0]
    pend = []

    class Send:
        def __init__(self, src, dst, landed, dev):
            i = n_used[0]
            n_used[0] += 1
            self.copy = pltpu.make_async_remote_copy(
                src_ref=src, dst_ref=dst, send_sem=ssem.at[i], recv_sem=rsem.at[i],
                device_id=dev, device_id_type=MESH,
            )
            self.twin = pltpu.make_async_remote_copy(
                src_ref=landed, dst_ref=landed, send_sem=ssem.at[i], recv_sem=rsem.at[i],
                device_id=dev, device_id_type=MESH,
            )

        def start(self):
            self.copy.start()
            pend.append(self.copy)

        def arrived(self):
            self.twin.wait_recv()

    row_loads, col_loads = [[], []], []
    half = D // 4
    for m, (r, cc) in enumerate(((rows_v, cols_v), (rows_o, cols_o))):
        cl = pltpu.make_async_copy(cc, cols.at[m], sem_cols.at[m])
        cl.start()
        col_loads.append(cl)
        for j in range(4):
            at = pl.ds(j * half, half)
            rl = pltpu.make_async_copy(r.at[:, at], rows.at[m, :, at], sem_rows.at[m, j])
            rl.start()
            row_loads[m].append(rl)

    barrier = pltpu.get_barrier_semaphore()
    for dz, dy in OFFSETS:
        pl.semaphore_signal(barrier, inc=1, device_id=plane(up(z, dz), up(y, dy)), device_id_type=MESH)
    pl.semaphore_signal(barrier, inc=1, device_id=mate, device_id_type=MESH)
    for q in range(1, ntp):
        pl.semaphore_signal(barrier, inc=1, device_id=along_x(q), device_id_type=MESH)

    for m, f in enumerate((fac_v, fac_o)):
        for s in range(2):
            k = 2 * h + s
            fg[m, z, y, c, k] = f[pl.ds(pl.multiple_of(k * QR, QR), QR), :]
    for m, w in enumerate((w_v, w_o)):
        for j in range(WS):
            wg[m, z, y, c, j] = w[pl.ds(j * WR, WR), :].astype(BF16)

    def line(buf, m, s, g, cc, k):
        return buf.at[m, :, dn(y, g), cc, k] if s == 0 else buf.at[m, dn(z, g), :, cc, k]

    def own(buf, m, s, d, k):
        return buf.at[m, dn(z, d), y, c, k] if s == 0 else buf.at[m, z, dn(y, d), c, k]

    def first_dev(s, d):
        return plane(up(z, d), y) if s == 0 else plane(z, up(y, d))

    def second_dev(s, d):
        return plane(z, up(y, d)) if s == 0 else plane(up(z, d), y)

    f1, f2, fx, fm, fxm = {}, {}, {}, {}, {}
    for m in range(2):
        for s in range(2):
            k, kx = 2 * h + s, 2 * (1 - h) + s
            for d in (2, 1, 3):
                f1[m, s, d] = Send(own(fg, m, s, 0, k), own(fg, m, s, 0, k), own(fg, m, s, d, k), first_dev(s, d))
                f2[m, s, d] = Send(line(fg, m, s, 0, c, k), line(fg, m, s, 0, c, k), line(fg, m, s, d, c, k), second_dev(s, d))
            for g in range(NZ):
                a, b = line(fg, m, s, g, c, k), line(fg, m, s, g, c, kx)
                fx[m, s, g] = Send(a, a, b, along_x(1 if s == 0 else -1))
                fm[m, s, g] = Send(a, a, line(fg, m, s, g, co, k), mate)
                fxm[m, s, g] = Send(b, b, line(fg, m, s, g, co, kx), mate)

    def f_first(m):
        for d in (2, 1, 3):
            for s in range(2):
                f1[m, s, d].start()

    def f_second(m):
        for s in range(2):
            for d in (1, 3, 2):
                f1[m, s, d].arrived()
            for d in (2, 1, 3):
                f2[m, s, d].start()
            fx[m, s, 0].start()
            fm[m, s, 0].start()

    def f_across(m, gs):
        for g in gs:
            for s in range(2):
                f2[m, s, g].arrived()
                fx[m, s, g].start()
                fm[m, s, g].start()

    def f_mate(m, gs):
        for g in gs:
            for s in range(2):
                fx[m, s, g].arrived()
                fxm[m, s, g].start()

    f_outs = []

    def f_done(m):
        for g in (0, 1, 3, 2):
            for s in range(2):
                fm[m, s, g].arrived()
                fxm[m, s, g].arrived()
        o = pltpu.make_async_copy(fg.at[m], fg_out.at[m], sem_out.at[m])
        o.start()
        f_outs.append(o)

    w1, w2, wm = {}, {}, {}
    for m in range(2):
        for j in range(WS):
            for d in (2, 1, 3):
                w1[m, j, d] = Send(own(wg, m, m, 0, j), own(wg, m, m, 0, j), own(wg, m, m, d, j), first_dev(m, d))
                w2[m, j, d] = Send(line(wg, m, m, 0, c, j), line(wg, m, m, 0, c, j), line(wg, m, m, d, c, j), second_dev(m, d))
        for g in range(NZ):
            def whole(cc, m=m, g=g):
                return wg.at[m, :, dn(y, g), cc] if m == 0 else wg.at[m, dn(z, g), :, cc]

            wm[m, g] = Send(whole(c), whole(c), whole(co), mate)

    def w_first():
        for j in range(WS):
            for d in (2, 1, 3):
                for m in range(2):
                    w1[m, j, d].start()

    def w_second(js):
        for j in js:
            for m in range(2):
                for d in (1, 3, 2):
                    w1[m, j, d].arrived()
            for d in (2, 1, 3):
                for m in range(2):
                    w2[m, j, d].start()

    def w_mate(gs):
        for g in gs:
            for m in range(2):
                if g:
                    for j in range(WS):
                        w2[m, j, g].arrived()
                wm[m, g].start()

    def turn_cols(m):
        col_loads[m].wait()
        for t in range(4):
            at = pl.ds(t * (T // 4), T // 4)
            cols_t[m, :, at] = cols[m, at, :].T

    def gradient(m, n):
        if n % (half // GN) == 0:
            row_loads[m][n // (half // GN)].wait()
        at = pl.ds(n * GN, GN)
        grad[m, :, at] = jnp.dot(cols_t[m], rows[m, :, at], preferred_element_type=F32).astype(BF16)

    def factor_of(m):
        return fg[m].reshape(D, R)

    sa, sb = {}, {}
    for m in range(2):
        sa[m] = Send(send_a.at[m], recv_a.at[m], recv_a.at[m], mate)
        for i, (dz, dy) in enumerate(OFFSETS):
            to = up(z, dz) * NZ + up(y, dy)
            sb[m, i] = Send(send_b.at[m, to], recv_b.at[m, i], recv_b.at[m, i], plane(up(z, dz), up(y, dy)))

    def project(m):
        f = factor_of(m)
        for b in range(2):
            w = R // 2
            pt = jnp.dot(grad[m], f[:, b * w:(b + 1) * w], preferred_element_type=F32)
            pf[m, pl.ds(b * NZ * NZ // 2, NZ * NZ // 2)] = pt.T.reshape(NZ * NZ // 2, NC, QR, C)
        send_a[m] = pf[m, :, co].astype(BF16)
        sa[m].start()

    def scatter(m):
        sa[m].arrived()
        send_b[m] = (pf[m, :, c] + recv_a[m].astype(F32)).astype(BF16)
        for i in range(len(OFFSETS)):
            sb[m, i].start()
        pg[m] = pf[m, chip, c] + recv_a[m, chip].astype(F32)

    dp, dm, dmo = {}, {}, {}
    for m in range(2):
        mine = dirg.at[m, chip, c]
        dmo[m] = Send(mine, mine, dirg.at[m, chip, co], mate)
        for i, (dz, dy) in enumerate(OFFSETS):
            frm = dn(z, dz) * NZ + dn(y, dy)
            dp[m, i] = Send(mine, mine, dirg.at[m, frm, c], plane(up(z, dz), up(y, dy)))
            dm[m, i] = Send(dirg.at[m, frm, c], dirg.at[m, frm, c], dirg.at[m, frm, co], mate)

    def moments(m, first, second, fnew, snew):
        tot = pg[m]
        for i in range(len(OFFSETS)):
            sb[m, i].arrived()
            tot = tot + recv_b[m, i].astype(F32)
        f = beta_first * first[...] + (1.0 - beta_first) * tot
        s = beta_second * second[...] + (1.0 - beta_second) * tot * tot
        dirg[m, chip, c] = (f / (jnp.sqrt(s) + tiny_eps)).astype(BF16)
        for i in range(len(OFFSETS)):
            dp[m, i].start()
        dmo[m].start()
        fnew[...] = f
        snew[...] = s

    def spread(m):
        for i in range(len(OFFSETS)):
            dp[m, i].arrived()
            dm[m, i].start()

    def gram_of(m):
        f = factor_of(m)
        ft = f.T
        g = jnp.dot(ft, f, preferred_element_type=F32)
        hi = g.astype(BF16)
        gram[m, 0] = hi
        gram[m, 1] = (g - hi.astype(F32)).astype(BF16)

    sq = {}
    for m in range(2):
        for q in range(1, ntp):
            sq[m, q] = Send(ss.at[m], ssg.at[m, q], ssg.at[m, q], along_x(q))

    def squares(m):
        dmo[m].arrived()
        for i in range(len(OFFSETS)):
            dm[m, i].arrived()
        d = dirg[m].reshape(R, C)
        e = jnp.dot(gram[m, 0], d, preferred_element_type=F32)
        e += jnp.dot(gram[m, 1], d, preferred_element_type=F32)
        p = jnp.sum((e * d.astype(F32)).reshape(R // 8, 8, C), axis=0)
        t = p[:, :128]
        for b in range(1, C // 128):
            t = t + p[:, b * 128:(b + 1) * 128]
        ss[m] = t
        for q in range(1, ntp):
            sq[m, q].start()
        o = pltpu.make_async_copy(dirg.at[m], dir_out.at[m], sem_out.at[4 + m])
        o.start()
        f_outs.append(o)

    def total(m):
        t = ss[m]
        for q in range(1, ntp):
            sq[m, q].arrived()
            t = t + ssg[m, q]
        ss_out[m] = t

    n_tiles = D // GN
    pl.semaphore_wait(barrier, len(OFFSETS) + 1 + ntp - 1)
    f_first(0)
    f_first(1)
    hooks = {
        (0, 1): lambda: f_second(0),
        (0, 2): lambda: f_second(1),
        (0, 3): lambda: w_first(),
        (1, 0): lambda: f_across(0, (1, 3)),
        (1, 1): lambda: f_across(0, (2,)),
        (1, 2): lambda: f_mate(0, (0,)),
        (1, 4): lambda: f_across(1, (1, 3)),
        (1, 5): lambda: (f_across(1, (2,)), w_second((0, 1))),
        (1, 6): lambda: f_mate(0, (1, 3)),
        (1, 7): lambda: (f_mate(0, (2,)), f_mate(1, (0,))),
    }
    for m in range(2):
        turn_cols(m)
        for n in range(n_tiles):
            gradient(m, n)
            if (m, n) in hooks:
                hooks[m, n]()
    f_done(0)
    project(0)
    f_mate(1, (1, 3))
    scatter(0)
    w_second((2,))
    gram_of(0)
    f_mate(1, (2,))
    f_done(1)
    project(1)
    moments(0, first_v, second_v, fnew_v, snew_v)
    scatter(1)
    w_second((3,))
    gram_of(1)
    spread(0)
    squares(0)
    w_mate((0,))
    moments(1, first_o, second_o, fnew_o, snew_o)
    w_mate((1, 3, 2))
    spread(1)
    squares(1)
    for g in range(NZ):
        for m in range(2):
            wm[m, g].arrived()
    for m in range(2):
        o = pltpu.make_async_copy(wg.at[m], wg_out.at[m], sem_out.at[2 + m])
        o.start()
        f_outs.append(o)
    total(0)
    total(1)
    for o in f_outs:
        o.wait()
    for p in pend:
        p.wait_send()


def finish_kernel(
    ntp,
    fg_in, wg_in, dir_in, ss_in, fac_v, fac_o, w_v, w_o, fn_v, sn_v, fn_o, sn_o,
    step_v, upd_v, fnew_v, snew_v, copy_v, step_o, upd_o, fnew_o, snew_o, copy_o,
    fg, wg, dirg, res, sem_f, sem_w, sem_d, sem_o,
):
    _, D, R = fg.shape
    C = wg.shape[2]
    CH = fg.shape[1] // sem_f.shape[1]
    n_ch = sem_f.shape[1]
    loads, outs = {}, []
    for m in range(2):
        loads["d", m] = pltpu.make_async_copy(dir_in.at[m], dirg.at[m], sem_d.at[m])
        loads["d", m].start()
        for b in range(n_ch):
            at = pl.ds(b * CH, CH)
            loads["f", m, b] = pltpu.make_async_copy(fg_in.at[m, at], fg.at[m, at], sem_f.at[m, b])
            loads["w", m, b] = pltpu.make_async_copy(wg_in.at[m, at], wg.at[m, at], sem_w.at[m, b])
            loads["f", m, b].start()
            loads["w", m, b].start()
    fnew_v[...] = fn_v[...]
    snew_v[...] = sn_v[...]
    fnew_o[...] = fn_o[...]
    snew_o[...] = sn_o[...]
    for m, (fac, w, step, upd, copy) in enumerate(
        ((fac_v, w_v, step_v, upd_v, copy_v), (fac_o, w_o, step_o, upd_o, copy_o))
    ):
        mean = jnp.sum(ss_in[m], keepdims=True) / (D * C * ntp)
        scale = step_rate / jnp.sqrt(mean + scale_floor)
        loads["d", m].wait()
        d = dirg[m]
        s = scale * jnp.dot(fac[...], d, preferred_element_type=F32)
        step[...] = s
        upd[...] = w[...] - s
        for b in range(n_ch):
            at = pl.ds(b * CH, CH)
            loads["f", m, b].wait()
            loads["w", m, b].wait()
            e = jnp.dot(fg[m, at], d, preferred_element_type=F32)
            res[m, at] = (wg[m, at].astype(F32) - scale * e).astype(BF16)
            o = pltpu.make_async_copy(res.at[m, at], copy.at[at], sem_o.at[m, b])
            o.start()
            outs.append(o)
    for o in outs:
        o.wait()


def local(
    n, ntp,
    model_input, value_cotan, mixer_cotan, head_output,
    value_weight, value_factor, value_first, value_second,
    output_weight, output_factor, output_first, output_second,
):
    T, D = model_input.shape
    C = value_cotan.shape[1]
    B, R = value_factor.shape
    k = value_first.shape[0]
    np_ = NZ * NZ
    vm = pl.BlockSpec(memory_space=pltpu.VMEM)
    hbm = pl.BlockSpec(memory_space=pl.ANY)
    mom = jax.ShapeDtypeStruct((k, C), F32)
    wide = jax.ShapeDtypeStruct((B, C), F32)
    full = jax.ShapeDtypeStruct((D, C), BF16)
    dma = pltpu.SemaphoreType.DMA
    fg_shape = (2, NZ, NZ, NC, NQ, B // NQ, R)
    wg_shape = (2, NZ, NZ, NC, WS, B // WS, C)
    dir_shape = (2, np_, NC, k, C)
    fn_v, sn_v, fn_o, sn_o, ss, fg, wg, dirg = pl.pallas_call(
        functools.partial(gather_kernel, ntp),
        out_shape=(mom,) * 4 + (
            jax.ShapeDtypeStruct((2, 8, 128), F32),
            jax.ShapeDtypeStruct(fg_shape, BF16),
            jax.ShapeDtypeStruct(wg_shape, BF16),
            jax.ShapeDtypeStruct(dir_shape, BF16),
        ),
        in_specs=[hbm] * 4 + [vm] * 8,
        out_specs=(vm,) * 5 + (hbm,) * 3,
        scratch_shapes=[
            pltpu.VMEM((2, T, D), BF16),
            pltpu.VMEM((2, T, C), BF16),
            pltpu.VMEM((2, C, T), BF16),
            pltpu.VMEM((2, C, D), BF16),
            pltpu.VMEM(fg_shape, BF16),
            pltpu.VMEM(wg_shape, BF16),
            pltpu.VMEM((2, np_, NC, k, C), F32),
            pltpu.VMEM((2, np_, k, C), BF16),
            pltpu.VMEM((2, np_, k, C), BF16),
            pltpu.VMEM((2, np_, k, C), BF16),
            pltpu.VMEM((2, np_ - 1, k, C), BF16),
            pltpu.VMEM((2, k, C), F32),
            pltpu.VMEM(dir_shape, BF16),
            pltpu.VMEM((2, 2, R, R), BF16),
            pltpu.VMEM((2, 8, 128), F32),
            pltpu.VMEM((2, ntp, 8, 128), F32),
            dma((2, 4)), dma((2,)), dma((6,)), dma((N_SEMS,)), dma((N_SEMS,)),
        ],
        compiler_params=pltpu.CompilerParams(
            collective_id=0, has_side_effects=True, vmem_limit_bytes=62_000_000
        ),
        name="gather",
    )(
        model_input, value_cotan, mixer_cotan, head_output,
        value_factor, output_factor, value_weight, output_weight,
        value_first, output_first, value_second, output_second,
    )
    n_ch = 4
    return pl.pallas_call(
        functools.partial(finish_kernel, ntp),
        out_shape=(wide, wide, mom, mom, full) * 2,
        in_specs=[hbm] * 3 + [vm] * 9,
        out_specs=(vm, vm, vm, vm, hbm) * 2,
        scratch_shapes=[
            pltpu.VMEM((2, D, R), BF16),
            pltpu.VMEM((2, D, C), BF16),
            pltpu.VMEM((2, R, C), BF16),
            pltpu.VMEM((2, D, C), BF16),
            dma((2, n_ch)), dma((2, n_ch)), dma((2,)), dma((2, n_ch)),
        ],
        compiler_params=pltpu.CompilerParams(vmem_limit_bytes=62_000_000),
        name="finish",
    )(
        fg.reshape(2, D, R), wg.reshape(2, D, C), dirg.reshape(2, R, C), ss,
        value_factor, output_factor, value_weight, output_weight,
        fn_v, sn_v, fn_o, sn_o,
    )


def solution(mesh):
    rows, both, full = P("fs", None), P("fs", "tp"), P(None, "tp")
    return jax.shard_map(
        functools.partial(local, mesh.shape["fs"], mesh.shape["tp"]),
        mesh=mesh,
        in_specs=(rows, both, rows, both) + (both, rows, both, both) * 2,
        out_specs=(both, both, both, both, full) * 2,
        check_vma=False,
    )
```

```python
import functools
import math

import jax
import jax.numpy as jnp
from jax import lax
from jax.experimental import pallas as pl
from jax.experimental.pallas import tpu as pltpu
from jax.sharding import PartitionSpec as P

beta_first = 0.8
beta_second = 0.9
step_rate = 0.02
scale_floor = 0.25
tiny_eps = 1e-08

MESH = pl.DeviceIdType.MESH
F32 = jnp.float32
BF16 = jnp.bfloat16
NZ = 4
NC = 2
NQ = 4
WS = 4
N_SEMS = 40
OFFSETS = sorted(
    [(a, b) for a in range(NZ) for b in range(NZ) if a or b],
    key=lambda o: -(min(o[0], NZ - o[0]) + min(o[1], NZ - o[1])),
)


def gather_kernel(
    ntp,
    rows_v, cols_v, rows_o, cols_o,
    fac_v, fac_o, w_v, w_o, first_v, first_o, second_v, second_o,
    fnew_v, snew_v, fnew_o, snew_o, ss_out, fg_out, wg_out, dir_out,
    rows, cols, cols_t, grad, fg, wg, pf, send_a, recv_a, send_b, recv_b, pg,
    dirg, gram, ss, ssg, sst, tally, wide, old, new,
    sem_rows, sem_cols, sem_out, sem_in, sem_new, ssem, rsem,
):
    me = lax.axis_index("fs")
    tp = lax.axis_index("tp")
    z, y, c = me // (NZ * NC), lax.rem(me // NC, NZ), lax.rem(me, NC)
    co = 1 - c
    chip = z * NZ + y
    h = lax.rem(tp, 2)
    T, D = rows_v.shape
    C = cols_v.shape[1]
    QR, R = fac_v.shape[1:]
    WR = w_v.shape[0] // WS

    def up(a, d):
        return lax.rem(a + d, NZ)

    def dn(a, d):
        return lax.rem(a + NZ - d, NZ)

    def plane(zz, yy):
        return ((zz * NZ + yy) * NC + c, tp)

    mate = (me - c + co, tp)

    def along_x(d):
        return (me, lax.rem(tp + ntp + d, ntp))

    row_bytes = 2 * tally.shape[1] * tally.shape[2]
    n_recv = [0]
    out_bytes = [0]

    def size(ref):
        return math.prod(ref.shape) * jnp.dtype(ref.dtype).itemsize // row_bytes

    class Group:
        def __init__(self):
            self.i, self.rows = n_recv[0], 0
            n_recv[0] += 1

        def arrived(self):
            all_of = tally.at[pl.ds(0, self.rows)]
            pltpu.make_async_remote_copy(
                src_ref=all_of, dst_ref=all_of, send_sem=ssem.at[0], recv_sem=rsem.at[self.i],
                device_id=mate, device_id_type=MESH,
            ).wait_recv()

    class Send:
        def __init__(self, src, dst, group, dev):
            if out_bytes[-1] + size(src) > tally.shape[0]:
                out_bytes.append(0)
            out_bytes[-1] += size(src)
            group.rows += size(src)
            self.copy = pltpu.make_async_remote_copy(
                src_ref=src, dst_ref=dst, send_sem=ssem.at[len(out_bytes) - 1], recv_sem=rsem.at[group.i],
                device_id=dev, device_id_type=MESH,
            )

        def start(self):
            self.copy.start()

    barrier = pltpu.get_barrier_semaphore()
    for dz, dy in OFFSETS:
        pl.semaphore_signal(barrier, inc=1, device_id=plane(up(z, dz), up(y, dy)), device_id_type=MESH)
    pl.semaphore_signal(barrier, inc=1, device_id=mate, device_id_type=MESH)
    for q in range(1, ntp):
        pl.semaphore_signal(barrier, inc=1, device_id=along_x(q), device_id_type=MESH)

    half = D // 4
    f_loads, w_loads, o_loads, row_loads, col_loads = [], [], [], [[], []], []
    for m, (r, cc, f, w, a, b) in enumerate((
        (rows_v, cols_v, fac_v, w_v, first_v, second_v), (rows_o, cols_o, fac_o, w_o, first_o, second_o)
    )):
        mine = pl.ds(2 * h, 2)
        f_loads.append(pltpu.make_async_copy(f.at[mine], fg.at[m, z, y, c, mine], sem_in.at[m]))
        w_loads.append(pltpu.make_async_copy(w, wide.at[m], sem_in.at[2 + m]))
        o_loads.append(pltpu.make_async_copy(a, old.at[m, 0], sem_in.at[4 + m]))
        o_loads.append(pltpu.make_async_copy(b, old.at[m, 1], sem_in.at[6 + m]))
        col_loads.append(pltpu.make_async_copy(cc, cols.at[m], sem_cols.at[m]))
        for j in range(4):
            at = pl.ds(j * half, half)
            row_loads[m].append(pltpu.make_async_copy(r.at[:, at], rows.at[m, :, at], sem_rows.at[m, j]))
    for x in (*f_loads, *w_loads, col_loads[0], row_loads[0][0], row_loads[0][1]):
        x.start()

    def line(buf, m, s, g, cc, k):
        return buf.at[m, :, dn(y, g), cc, k] if s == 0 else buf.at[m, dn(z, g), :, cc, k]

    def own(buf, m, s, d, k):
        return buf.at[m, dn(z, d), y, c, k] if s == 0 else buf.at[m, z, dn(y, d), c, k]

    def first_dev(s, d):
        return plane(up(z, d), y) if s == 0 else plane(z, up(y, d))

    def second_dev(s, d):
        return plane(z, up(y, d)) if s == 0 else plane(up(z, d), y)

    f1, f2, fx, fm, fxm = {}, {}, {}, {}, {}
    f1_in, f2_in, fx_in, fm_in = {}, {}, {}, {}
    for m in range(2):
        f1_in[m], fm_in[m] = Group(), Group()
        f2_in[m, 1] = f2_in[m, 3] = Group()
        f2_in[m, 2] = Group()
        fx_in[m, 0], fx_in[m, 2] = Group(), Group()
        fx_in[m, 1] = fx_in[m, 3] = Group()
        for s in range(2):
            k, kx = 2 * h + s, 2 * (1 - h) + s
            for d in (2, 1, 3):
                f1[m, s, d] = Send(own(fg, m, s, 0, k), own(fg, m, s, 0, k), f1_in[m], first_dev(s, d))
                f2[m, s, d] = Send(line(fg, m, s, 0, c, k), line(fg, m, s, 0, c, k), f2_in[m, d], second_dev(s, d))
            for g in range(NZ):
                a, b = line(fg, m, s, g, c, k), line(fg, m, s, g, c, kx)
                fx[m, s, g] = Send(a, a, fx_in[m, g], along_x(1 if s == 0 else -1))
                fm[m, s, g] = Send(a, a, fm_in[m], mate)
                fxm[m, s, g] = Send(b, b, fm_in[m], mate)

    def f_first(m):
        for d in (2, 1, 3):
            for s in range(2):
                f1[m, s, d].start()

    def f_second(m):
        f1_in[m].arrived()
        for d in (1, 3, 2):
            for s in range(2):
                f2[m, s, d].start()
        for s in range(2):
            fx[m, s, 0].start()
            fm[m, s, 0].start()

    def f_across(m, gs):
        f2_in[m, gs[0]].arrived()
        for g in gs:
            for s in range(2):
                fx[m, s, g].start()
                fm[m, s, g].start()

    def f_mate(m, gs):
        fx_in[m, gs[0]].arrived()
        for g in gs:
            for s in range(2):
                fxm[m, s, g].start()

    f_outs = []

    def f_done(m):
        fm_in[m].arrived()
        o = pltpu.make_async_copy(fg.at[m], fg_out.at[m], sem_out.at[m])
        o.start()
        f_outs.append(o)

    w1, w2, w3, wm = {}, {}, {}, {}

    def part(m, j, g, b):
        two = pl.ds(2 * b, 2)
        return wg.at[m, two, dn(y, g), c, j] if m == 0 else wg.at[m, dn(z, g), two, c, j]

    w1_in, w3_in, wm_in = Group(), Group(), Group()
    w2_in = {}
    for j in range(WS):
        w2_in[j] = Group()
        for m in range(2):
            for d in (2, 1, 3):
                w1[m, j, d] = Send(own(wg, m, m, 0, j), own(wg, m, m, 0, j), w1_in, first_dev(m, d))
            for d in (1, 3):
                w2[m, j, d] = Send(line(wg, m, m, 0, c, j), line(wg, m, m, 0, c, j), w2_in[j], second_dev(m, d))
                b = d // 2
                w3[m, j, d] = Send(part(m, j, d, b), part(m, j, d, b), w3_in, second_dev(m, d))
    for m in range(2):
        for g in range(NZ):
            a = wg.at[m, :, dn(y, g), c] if m == 0 else wg.at[m, dn(z, g), :, c]
            wm[m, g] = Send(a, a, wm_in, mate)

    def w_own():
        for m in range(2):
            w_loads[m].wait()
            wg[m, z, y, c] = wide[m].reshape(WS, WR, C).astype(BF16)

    def w_first():
        for j in range(WS):
            for d in (2, 1, 3):
                for m in range(2):
                    w1[m, j, d].start()

    def w_second(js):
        if js[0] == 0:
            w1_in.arrived()
        for j in js:
            for d in (1, 3):
                for m in range(2):
                    w2[m, j, d].start()

    def w_third(js):
        for j in js:
            w2_in[j].arrived()
            for d in (1, 3):
                for m in range(2):
                    w3[m, j, d].start()

    def w_mate(gs):
        if gs[0] == 2:
            w3_in.arrived()
        for g in gs:
            for m in range(2):
                wm[m, g].start()

    def turn_cols(m):
        col_loads[m].wait()
        for t in range(4):
            at = pl.ds(t * (T // 4), T // 4)
            cols_t[m, :, at] = cols[m, at, :].T

    def gradient(m, n):
        j, b = n // 2, n % 2
        if b == 0:
            row_loads[m][j].wait()
        at, up_to = pl.ds(j * half, half), pl.ds(b * (C // 2), C // 2)
        grad[m, up_to, at] = jnp.dot(cols_t[m, up_to], rows[m, :, at], preferred_element_type=F32).astype(BF16)

    def factor_of(m):
        return fg[m].reshape(D, R)

    sa, sb, sa_in, sb_in = {}, {}, {}, {}
    for m in range(2):
        sa_in[m], sb_in[m] = Group(), Group()
        sa[m] = Send(send_a.at[m], recv_a.at[m], sa_in[m], mate)
        for i, (dz, dy) in enumerate(OFFSETS):
            to = up(z, dz) * NZ + up(y, dy)
            sb[m, i] = Send(send_b.at[m, to], recv_b.at[m, i], sb_in[m], plane(up(z, dz), up(y, dy)))

    def project(m):
        pt = jnp.dot(grad[m], factor_of(m), preferred_element_type=F32)
        pf[m] = pt.T.reshape(NZ * NZ, NC, QR, C)
        send_a[m] = pf[m, :, co].astype(BF16)
        sa[m].start()

    def scatter(m):
        sa_in[m].arrived()
        send_b[m] = (pf[m, :, c] + recv_a[m].astype(F32)).astype(BF16)
        for i in range(len(OFFSETS)):
            sb[m, i].start()
        pg[m] = pf[m, chip, c] + recv_a[m, chip].astype(F32)

    dp, dm, dp_in, dm_in = {}, {}, {}, {}
    for m in range(2):
        dp_in[m], dm_in[m] = Group(), Group()
        mine = dirg.at[m, chip, c]
        for i, (dz, dy) in enumerate(OFFSETS):
            dp[m, i] = Send(mine, mine, dp_in[m], plane(up(z, dz), up(y, dy)))
        dm[m] = Send(dirg.at[m, :, c], dirg.at[m, :, c], dm_in[m], mate)

    def moments(m, fnew, snew):
        tot = pg[m]
        o_loads[2 * m].wait()
        o_loads[2 * m + 1].wait()
        sb_in[m].arrived()
        for i in range(len(OFFSETS)):
            tot = tot + recv_b[m, i].astype(F32)
        f = beta_first * old[m, 0] + (1.0 - beta_first) * tot
        s = beta_second * old[m, 1] + (1.0 - beta_second) * tot * tot
        dirg[m, chip, c] = (f / (jnp.sqrt(s) + tiny_eps)).astype(BF16)
        for i in range(len(OFFSETS)):
            dp[m, i].start()
        new[m, 0] = f
        new[m, 1] = s
        for i, out in enumerate((fnew, snew)):
            o = pltpu.make_async_copy(new.at[m, i], out, sem_new.at[m, i])
            o.start()
            f_outs.append(o)

    def spread(m):
        dp_in[m].arrived()
        dm[m].start()

    def gram_of(m):
        f = factor_of(m)
        ft = f.T
        g = jnp.dot(ft, f, preferred_element_type=F32)
        hi = g.astype(BF16)
        gram[m, 0] = hi
        gram[m, 1] = (g - hi.astype(F32)).astype(BF16)

    sq, sq_in = {}, {}
    for m in range(2):
        sq_in[m] = Group()
        for q in range(1, ntp):
            sq[m, q] = Send(ss.at[m], ssg.at[m, q], sq_in[m], along_x(q))

    def squares(m):
        dm_in[m].arrived()
        d = dirg[m].reshape(R, C)
        e = jnp.dot(gram[m, 0], d, preferred_element_type=F32)
        e += jnp.dot(gram[m, 1], d, preferred_element_type=F32)
        p = jnp.sum((e * d.astype(F32)).reshape(R // 8, 8, C), axis=0)
        t = p[:, :128]
        for b in range(1, C // 128):
            t = t + p[:, b * 128:(b + 1) * 128]
        ss[m] = t
        for q in range(1, ntp):
            sq[m, q].start()
        o = pltpu.make_async_copy(dirg.at[m], dir_out.at[m], sem_out.at[4 + m])
        o.start()
        f_outs.append(o)

    def total(m):
        t = ss[m]
        sq_in[m].arrived()
        for q in range(1, ntp):
            t = t + ssg[m, q]
        sst[m] = t
        o = pltpu.make_async_copy(sst.at[m], ss_out.at[m], sem_new.at[m, 2])
        o.start()
        f_outs.append(o)

    for x in f_loads:
        x.wait()
    pl.semaphore_wait(barrier, len(OFFSETS) + 1 + ntp - 1)
    f_first(0)
    f_first(1)
    w_own()
    w_first()
    for x in (row_loads[0][2], row_loads[0][3], col_loads[1], *o_loads):
        x.start()

    def more_rows():
        for x in row_loads[1]:
            x.start()

    hooks = {
        (0, 1): lambda: (more_rows(), f_second(0)),
        (0, 2): lambda: f_second(1),
        (0, 3): lambda: w_second(range(WS)),
        (0, 7): lambda: f_across(0, (1, 3)),
        (1, 0): lambda: (f_across(0, (2,)), f_mate(0, (0,))),
        (1, 2): lambda: (f_across(1, (1, 3)), f_mate(1, (0,))),
        (1, 4): lambda: (f_mate(0, (1, 3)), f_across(1, (2,))),
        (1, 6): lambda: (f_mate(0, (2,)), w_third((0, 1))),
        (1, 7): lambda: f_mate(1, (1, 3)),
    }
    for m in range(2):
        turn_cols(m)
        for n in range(8):
            gradient(m, n)
            if (m, n) in hooks:
                hooks[m, n]()
    f_done(0)
    project(0)
    f_mate(1, (2,))
    w_third((2, 3))
    scatter(0)
    f_done(1)
    project(1)
    gram_of(0)
    scatter(1)
    moments(0, fnew_v, snew_v)
    w_mate((0, 1, 3))
    gram_of(1)
    spread(0)
    moments(1, fnew_o, snew_o)
    squares(0)
    w_mate((2,))
    spread(1)
    squares(1)
    wm_in.arrived()
    for m in range(2):
        o = pltpu.make_async_copy(wg.at[m], wg_out.at[m], sem_out.at[2 + m])
        o.start()
        f_outs.append(o)
    total(0)
    total(1)
    for o in f_outs:
        o.wait()
    for i, n in enumerate(out_bytes):
        all_of = tally.at[pl.ds(0, n)]
        pltpu.make_async_remote_copy(
            src_ref=all_of, dst_ref=all_of, send_sem=ssem.at[i], recv_sem=rsem.at[0],
            device_id=mate, device_id_type=MESH,
        ).wait_send()


def finish_kernel(
    ntp,
    fg_in, wg_in, dir_in, ss_in, fac_v, fac_o, w_v, w_o, fn_v, sn_v, fn_o, sn_o,
    step_v, upd_v, fnew_v, snew_v, copy_v, step_o, upd_o, fnew_o, snew_o, copy_o,
    fg, wg, dirg, res, fac, w, mo, ss, st, up, sem_f, sem_w, sem_s, sem_o, sem_p,
):
    _, D, R = fg.shape
    C = wg.shape[2]
    n_ch = sem_f.shape[1]
    CH = D // n_ch
    loads, outs = {}, []

    def load(key, src, dst, sem):
        loads[key] = pltpu.make_async_copy(src, dst, sem)
        loads[key].start()

    def store(src, dst, sem):
        o = pltpu.make_async_copy(src, dst, sem)
        o.start()
        outs.append(o)

    load("s", ss_in, ss, sem_s.at[0])
    mo_out = ((fnew_v, snew_v), (fnew_o, snew_o))
    for m in range(2):
        load(("d", m), dir_in.at[m], dirg.at[m], sem_s.at[1 + m])
        for b in range(n_ch):
            at = pl.ds(b * CH, CH)
            load(("f", m, b), fg_in.at[m, at], fg.at[m, at], sem_f.at[m, b])
            load(("w", m, b), wg_in.at[m, at], wg.at[m, at], sem_w.at[m, b])
        load(("k", m), (fac_v, fac_o)[m], fac.at[m], sem_s.at[3 + m])
        load(("g", m), (w_v, w_o)[m], w.at[m], sem_s.at[5 + m])
        for i in range(2):
            load(("m", m, i), ((fn_v, sn_v), (fn_o, sn_o))[m][i], mo.at[m, i], sem_p.at[m, i])
    loads["s"].wait()
    for m, (step, upd, copy) in enumerate(((step_v, upd_v, copy_v), (step_o, upd_o, copy_o))):
        mean = jnp.sum(ss[m], keepdims=True) / (D * C * ntp)
        scale = step_rate / jnp.sqrt(mean + scale_floor)
        loads["d", m].wait()
        d = dirg[m]
        for b in range(n_ch):
            at = pl.ds(b * CH, CH)
            loads["f", m, b].wait()
            loads["w", m, b].wait()
            with jax.named_scope(f"fin_{m}_{b}"):
                e = jnp.dot(fg[m, at], d, preferred_element_type=F32)
                res[m, at] = (wg[m, at].astype(F32) - scale * e).astype(BF16)
            store(res.at[m, at], copy.at[at], sem_o.at[m, b])
        for i in range(2):
            loads["m", m, i].wait()
            store(mo.at[m, i], mo_out[m][i], sem_p.at[m, i])
        loads["k", m].wait()
        loads["g", m].wait()
        s = scale * jnp.dot(fac[m], d, preferred_element_type=F32)
        st[m] = s
        up[m] = w[m] - s
        store(st.at[m], step, sem_s.at[7 + m])
        store(up.at[m], upd, sem_s.at[9 + m])
    for o in outs:
        o.wait()


def local(
    n, ntp,
    model_input, value_cotan, mixer_cotan, head_output,
    value_weight, value_factor, value_first, value_second,
    output_weight, output_factor, output_first, output_second,
):
    T, D = model_input.shape
    C = value_cotan.shape[1]
    B, R = value_factor.shape
    k = value_first.shape[0]
    np_ = NZ * NZ
    hbm = pl.BlockSpec(memory_space=pl.ANY)
    mom = jax.ShapeDtypeStruct((k, C), F32)
    wide = jax.ShapeDtypeStruct((B, C), F32)
    full = jax.ShapeDtypeStruct((D, C), BF16)
    dma = pltpu.SemaphoreType.DMA
    fg_shape = (2, NZ, NZ, NC, NQ, B // NQ, R)
    wg_shape = (2, NZ, NZ, NC, WS, B // WS, C)
    dir_shape = (2, np_, NC, k, C)
    fn_v, sn_v, fn_o, sn_o, ss, fg, wg, dirg = pl.pallas_call(
        functools.partial(gather_kernel, ntp),
        out_shape=(mom,) * 4 + (
            jax.ShapeDtypeStruct((2, 8, 128), F32),
            jax.ShapeDtypeStruct(fg_shape, BF16),
            jax.ShapeDtypeStruct(wg_shape, BF16),
            jax.ShapeDtypeStruct(dir_shape, BF16),
        ),
        in_specs=[hbm] * 12,
        out_specs=(hbm,) * 8,
        scratch_shapes=[
            pltpu.VMEM((2, T, D), BF16),
            pltpu.VMEM((2, T, C), BF16),
            pltpu.VMEM((2, C, T), BF16),
            pltpu.VMEM((2, C, D), BF16),
            pltpu.VMEM(fg_shape, BF16),
            pltpu.VMEM(wg_shape, BF16),
            pltpu.VMEM((2, np_, NC, k, C), F32),
            pltpu.VMEM((2, np_, k, C), BF16),
            pltpu.VMEM((2, np_, k, C), BF16),
            pltpu.VMEM((2, np_, k, C), BF16),
            pltpu.VMEM((2, np_ - 1, k, C), BF16),
            pltpu.VMEM((2, k, C), F32),
            pltpu.VMEM(dir_shape, BF16),
            pltpu.VMEM((2, 2, R, R), BF16),
            pltpu.VMEM((2, 8, 128), F32),
            pltpu.VMEM((2, ntp, 8, 128), F32),
            pltpu.VMEM((2, 8, 128), F32),
            pltpu.VMEM((512, 16, 128), BF16),
            pltpu.VMEM((2, B, C), F32),
            pltpu.VMEM((2, 2, k, C), F32),
            pltpu.VMEM((2, 2, k, C), F32),
            dma((2, 4)), dma((2,)), dma((6,)), dma((8,)), dma((2, 3)), dma((N_SEMS,)), dma((N_SEMS,)),
        ],
        compiler_params=pltpu.CompilerParams(
            collective_id=0, has_side_effects=True, vmem_limit_bytes=62_000_000
        ),
        name="gather",
    )(
        model_input, value_cotan, mixer_cotan, head_output,
        value_factor.reshape(NQ, B // NQ, R), output_factor.reshape(NQ, B // NQ, R), value_weight, output_weight,
        value_first, output_first, value_second, output_second,
    )
    n_ch = 4
    return pl.pallas_call(
        functools.partial(finish_kernel, ntp),
        out_shape=(wide, wide, mom, mom, full) * 2,
        in_specs=[hbm] * 12,
        out_specs=(hbm,) * 10,
        scratch_shapes=[
            pltpu.VMEM((2, D, R), BF16),
            pltpu.VMEM((2, D, C), BF16),
            pltpu.VMEM((2, R, C), BF16),
            pltpu.VMEM((2, D, C), BF16),
            pltpu.VMEM((2, B, R), BF16),
            pltpu.VMEM((2, B, C), F32),
            pltpu.VMEM((2, 2, k, C), F32),
            pltpu.VMEM((2, 8, 128), F32),
            pltpu.VMEM((2, B, C), F32),
            pltpu.VMEM((2, B, C), F32),
            dma((2, n_ch)), dma((2, n_ch)), dma((11,)), dma((2, n_ch)), dma((2, 2)),
        ],
        compiler_params=pltpu.CompilerParams(vmem_limit_bytes=62_000_000),
        name="finish",
    )(
        fg.reshape(2, D, R), wg.reshape(2, D, C), dirg.reshape(2, R, C), ss,
        value_factor, output_factor, value_weight, output_weight,
        fn_v, sn_v, fn_o, sn_o,
    )


def solution(mesh):
    rows, both, full = P("fs", None), P("fs", "tp"), P(None, "tp")
    return jax.shard_map(
        functools.partial(local, mesh.shape["fs"], mesh.shape["tp"]),
        mesh=mesh,
        in_specs=(rows, both, rows, both) + (both, rows, both, both) * 2,
        out_specs=(both, both, both, both, full) * 2,
        check_vma=False,
    )
```

```python
import functools
import math

import jax
import jax.numpy as jnp
from jax import lax
from jax.experimental import pallas as pl
from jax.experimental.pallas import tpu as pltpu
from jax.sharding import PartitionSpec as P

beta_first = 0.8
beta_second = 0.9
step_rate = 0.02
scale_floor = 0.25
tiny_eps = 1e-08

MESH = pl.DeviceIdType.MESH
F32 = jnp.float32
BF16 = jnp.bfloat16
NZ = 4
NC = 2
NQ = 4
WS = 4
NH = 2
N_SEMS = 64
OFFSETS = sorted(
    [(a, b) for a in range(NZ) for b in range(NZ) if a or b],
    key=lambda o: -(min(o[0], NZ - o[0]) + min(o[1], NZ - o[1])),
)


def gather_kernel(
    ntp,
    rows_v, cols_v, rows_o, cols_o,
    fac_v, fac_o, w_v, w_o, first_v, first_o, second_v, second_o,
    new, sst, wg, ex,
    rows, cols, cols_t, grad, fg, pf, send_a, recv_a, send_b, recv_b, pg,
    dirg, gram, ss, ssg, tally, wide, old,
    sem_rows, sem_cols, sem_in, ssem, rsem,
):
    me = lax.axis_index("fs")
    tp = lax.axis_index("tp")
    z, y, c = me // (NZ * NC), lax.rem(me // NC, NZ), lax.rem(me, NC)
    co = 1 - c
    chip = z * NZ + y
    h = lax.rem(tp, 2)
    T, D = rows_v.shape
    C = cols_v.shape[1]
    QR, R = fac_v.shape[1:]
    WR = w_v.shape[0] // WS

    def up(a, d):
        return lax.rem(a + d, NZ)

    def dn(a, d):
        return lax.rem(a + NZ - d, NZ)

    def plane(zz, yy):
        return ((zz * NZ + yy) * NC + c, tp)

    mate = (me - c + co, tp)

    def along_x(d):
        return (me, lax.rem(tp + ntp + d, ntp))

    row_bytes = 2 * tally.shape[1] * tally.shape[2]
    n_recv = [0]
    out_bytes = [0]

    def size(ref):
        return math.prod(ref.shape) * jnp.dtype(ref.dtype).itemsize // row_bytes

    class Group:
        def __init__(self):
            self.i, self.rows = n_recv[0], 0
            n_recv[0] += 1

        def arrived(self):
            all_of = tally.at[pl.ds(0, self.rows)]
            pltpu.make_async_remote_copy(
                src_ref=all_of, dst_ref=all_of, send_sem=ssem.at[0], recv_sem=rsem.at[self.i],
                device_id=mate, device_id_type=MESH,
            ).wait_recv()

    class Send:
        def __init__(self, src, dst, group, dev):
            if out_bytes[-1] + size(src) > tally.shape[0]:
                out_bytes.append(0)
            out_bytes[-1] += size(src)
            group.rows += size(src)
            self.copy = pltpu.make_async_remote_copy(
                src_ref=src, dst_ref=dst, send_sem=ssem.at[len(out_bytes) - 1], recv_sem=rsem.at[group.i],
                device_id=dev, device_id_type=MESH,
            )

        def start(self):
            self.copy.start()

    barrier = pltpu.get_barrier_semaphore()
    for dz, dy in OFFSETS:
        pl.semaphore_signal(barrier, inc=1, device_id=plane(up(z, dz), up(y, dy)), device_id_type=MESH)
    pl.semaphore_signal(barrier, inc=1, device_id=mate, device_id_type=MESH)
    for q in range(1, ntp):
        pl.semaphore_signal(barrier, inc=1, device_id=along_x(q), device_id_type=MESH)

    half = D // 4
    f_loads, w_loads, o_loads, row_loads, col_loads = [], [], [], [[], []], []
    for m, (r, cc, f, w, a, b) in enumerate((
        (rows_v, cols_v, fac_v, w_v, first_v, second_v), (rows_o, cols_o, fac_o, w_o, first_o, second_o)
    )):
        mine = pl.ds(2 * h, 2)
        f_loads.append(pltpu.make_async_copy(f.at[mine], fg.at[m, z, y, c, mine], sem_in.at[m]))
        w_loads.append(pltpu.make_async_copy(w, wide.at[m], sem_in.at[2 + m]))
        o_loads.append(pltpu.make_async_copy(a, old.at[m, 0], sem_in.at[4 + m]))
        o_loads.append(pltpu.make_async_copy(b, old.at[m, 1], sem_in.at[6 + m]))
        col_loads.append(pltpu.make_async_copy(cc, cols.at[m], sem_cols.at[m]))
        for j in range(4):
            at = pl.ds(j * half, half)
            row_loads[m].append(pltpu.make_async_copy(r.at[:, at], rows.at[m, :, at], sem_rows.at[m, j]))
    for x in (*f_loads, *w_loads, col_loads[0], row_loads[0][0], row_loads[0][1]):
        x.start()

    def line(buf, m, s, g, cc, k):
        return buf.at[m, :, dn(y, g), cc, k] if s == 0 else buf.at[m, dn(z, g), :, cc, k]

    def own(buf, m, s, d, k):
        return buf.at[m, dn(z, d), y, c, k] if s == 0 else buf.at[m, z, dn(y, d), c, k]

    def first_dev(s, d):
        return plane(up(z, d), y) if s == 0 else plane(z, up(y, d))

    def second_dev(s, d):
        return plane(z, up(y, d)) if s == 0 else plane(up(z, d), y)

    f1, f2, fx, fm, fxm = {}, {}, {}, {}, {}
    f1_in, f2_in, fx_in, fm_in = {}, {}, {}, {}
    for m in range(2):
        f1_in[m], fm_in[m] = Group(), Group()
        f2_in[m, 1] = f2_in[m, 3] = Group()
        f2_in[m, 2] = Group()
        fx_in[m, 0], fx_in[m, 2] = Group(), Group()
        fx_in[m, 1] = fx_in[m, 3] = Group()
        for s in range(2):
            k, kx = 2 * h + s, 2 * (1 - h) + s
            for d in (2, 1, 3):
                f1[m, s, d] = Send(own(fg, m, s, 0, k), own(fg, m, s, 0, k), f1_in[m], first_dev(s, d))
                f2[m, s, d] = Send(line(fg, m, s, 0, c, k), line(fg, m, s, 0, c, k), f2_in[m, d], second_dev(s, d))
            for g in range(NZ):
                a, b = line(fg, m, s, g, c, k), line(fg, m, s, g, c, kx)
                if g == 2:
                    o = line(fg, m, s, 0, c, kx)
                    fx[m, s, g] = Send(o, o, fx_in[m, g], second_dev(s, 2))
                else:
                    fx[m, s, g] = Send(a, a, fx_in[m, g], along_x(1 if s == 0 else -1))
                fm[m, s, g] = Send(a, a, fm_in[m], mate)
                fxm[m, s, g] = Send(b, b, fm_in[m], mate)

    def f_first(m):
        for d in (2, 1, 3):
            for s in range(2):
                f1[m, s, d].start()

    def f_second(m):
        f1_in[m].arrived()
        for d in (1, 3, 2):
            for s in range(2):
                f2[m, s, d].start()
        for s in range(2):
            fx[m, s, 0].start()
            fm[m, s, 0].start()

    def f_across(m, gs):
        f2_in[m, gs[0]].arrived()
        for g in gs:
            for s in range(2):
                if g != 2:
                    fx[m, s, g].start()
                fm[m, s, g].start()

    def f_mate(m, gs):
        fx_in[m, gs[0]].arrived()
        for g in gs:
            for s in range(2):
                if g == 0:
                    fx[m, s, 2].start()
                fxm[m, s, g].start()

    def f_done(m):
        fm_in[m].arrived()

    w1, w2, w3, wm = {}, {}, {}, {}

    def part(m, j, g, b):
        two = pl.ds(2 * b, 2)
        return wg.at[m, two, dn(y, g), c, j] if m == 0 else wg.at[m, dn(z, g), two, c, j]

    w1_in, w3_in, wm_in = Group(), Group(), Group()
    w2_in = {}
    for j in range(WS):
        w2_in[j] = Group()
        for m in range(2):
            for d in (2, 1, 3):
                w1[m, j, d] = Send(own(wg, m, m, 0, j), own(wg, m, m, 0, j), w1_in, first_dev(m, d))
            for d in (1, 3):
                w2[m, j, d] = Send(line(wg, m, m, 0, c, j), line(wg, m, m, 0, c, j), w2_in[j], second_dev(m, d))
                b = d // 2
                w3[m, j, d] = Send(part(m, j, d, b), part(m, j, d, b), w3_in, second_dev(m, d))
    for m in range(2):
        for g in range(NZ):
            a = wg.at[m, :, dn(y, g), c] if m == 0 else wg.at[m, dn(z, g), :, c]
            wm[m, g] = Send(a, a, wm_in, mate)

    def w_own():
        for m in range(2):
            w_loads[m].wait()
            wg[m, z, y, c] = wide[m].reshape(WS, WR, C).astype(BF16)

    def w_first():
        for j in range(WS):
            for d in (2, 1, 3):
                for m in range(2):
                    w1[m, j, d].start()

    def w_second(js):
        if js[0] == 0:
            w1_in.arrived()
        for j in js:
            for d in (1, 3):
                for m in range(2):
                    w2[m, j, d].start()

    def w_have(js):
        for j in js:
            w2_in[j].arrived()

    def w_third(js):
        for j in js:
            for d in (1, 3):
                for m in range(2):
                    w3[m, j, d].start()

    def w_mate(gs):
        if gs[0] == 2:
            w3_in.arrived()
        for g in gs:
            for m in range(2):
                wm[m, g].start()

    def turn_cols(m):
        col_loads[m].wait()
        for t in range(4):
            at = pl.ds(t * (T // 4), T // 4)
            cols_t[m, :, at] = cols[m, at, :].T

    def gradient(m, n):
        j, b = n // 2, n % 2
        if b == 0:
            row_loads[m][j].wait()
        at, up_to = pl.ds(j * half, half), pl.ds(b * (C // 2), C // 2)
        grad[m, up_to, at] = jnp.dot(cols_t[m, up_to], rows[m, :, at], preferred_element_type=F32).astype(BF16)

    def factor_of(m):
        return fg[m].reshape(D, R)

    CW = C // NH
    sa, sb, sa_in, sb_in = {}, {}, {}, {}
    dp, dp_in, dm, dm_in = {}, {}, {}, {}
    for m in range(2):
        for b in range(NH):
            p = m, b
            sa_in[p], sb_in[p], dp_in[p], dm_in[p] = Group(), Group(), Group(), Group()
            sa[p] = Send(send_a.at[m, b], recv_a.at[m, b], sa_in[p], mate)
            mine = dirg.at[m, b, chip, c]
            for i, (dz, dy) in enumerate(OFFSETS):
                to = up(z, dz) * NZ + up(y, dy)
                dev = plane(up(z, dz), up(y, dy))
                sb[m, b, i] = Send(send_b.at[m, b, to], recv_b.at[m, b, i], sb_in[p], dev)
                dp[m, b, i] = Send(mine, mine, dp_in[p], dev)
            dm[p] = Send(dirg.at[m, b, :, c], dirg.at[m, b, :, c], dm_in[p], mate)

    def project(m, b):
        pt = jnp.dot(grad[m, pl.ds(b * CW, CW)], factor_of(m), preferred_element_type=F32)
        pf[m, b] = pt.T.reshape(NZ * NZ, NC, QR, CW)
        send_a[m, b] = pf[m, b, :, co].astype(BF16)
        sa[m, b].start()

    def scatter(m, b):
        sa_in[m, b].arrived()
        send_b[m, b] = (pf[m, b, :, c] + recv_a[m, b].astype(F32)).astype(BF16)
        for i in range(len(OFFSETS)):
            sb[m, b, i].start()
        pg[m, b] = pf[m, b, chip, c] + recv_a[m, b, chip].astype(F32)

    def moments(m, b):
        tot = pg[m, b]
        at = pl.ds(b * CW, CW)
        if b == 0:
            o_loads[2 * m].wait()
            o_loads[2 * m + 1].wait()
        sb_in[m, b].arrived()
        for i in range(len(OFFSETS)):
            tot = tot + recv_b[m, b, i].astype(F32)
        f = beta_first * old[m, 0, :, at] + (1.0 - beta_first) * tot
        s = beta_second * old[m, 1, :, at] + (1.0 - beta_second) * tot * tot
        dirg[m, b, chip, c] = (f / (jnp.sqrt(s) + tiny_eps)).astype(BF16)
        for i in range(len(OFFSETS)):
            dp[m, b, i].start()
        new[m, 0, :, at] = f
        new[m, 1, :, at] = s

    def spread(m, b):
        dp_in[m, b].arrived()
        dm[m, b].start()

    def direction_of(m):
        return jnp.concatenate([dirg[m, b].reshape(R, CW) for b in range(NH)], axis=1)

    def gram_of(m):
        f = factor_of(m)
        ft = f.T
        g = jnp.dot(ft, f, preferred_element_type=F32)
        hi = g.astype(BF16)
        gram[m, 0] = hi
        gram[m, 1] = (g - hi.astype(F32)).astype(BF16)

    sq, sq_in = {}, {}
    for m in range(2):
        sq_in[m] = Group()
        for q in range(1, ntp):
            sq[m, q] = Send(ss.at[m], ssg.at[m, q], sq_in[m], along_x(q))

    def squares(m):
        for b in range(NH):
            dm_in[m, b].arrived()
        d = direction_of(m)
        e = jnp.dot(gram[m, 0], d, preferred_element_type=F32)
        e += jnp.dot(gram[m, 1], d, preferred_element_type=F32)
        p = jnp.sum((e * d.astype(F32)).reshape(R // 8, 8, C), axis=0)
        t = p[:, :128]
        for b in range(1, C // 128):
            t = t + p[:, b * 128:(b + 1) * 128]
        ss[m] = t
        for q in range(1, ntp):
            sq[m, q].start()

    def expand(m):
        d = direction_of(m)
        f = fg.at[m]
        for b in range(NZ):
            ex[m, pl.ds(b * NZ * NC, NZ * NC)] = jnp.dot(
                f[b].reshape(D // NZ, R), d, preferred_element_type=F32
            ).reshape(NZ * NC, NQ * QR, C)

    def total(m):
        t = ss[m]
        sq_in[m].arrived()
        for q in range(1, ntp):
            t = t + ssg[m, q]
        sst[m] = t

    for x in f_loads:
        x.wait()
    pl.semaphore_wait(barrier, len(OFFSETS) + 1 + ntp - 1)
    f_first(0)
    f_first(1)
    w_own()
    w_first()
    for x in (row_loads[0][2], row_loads[0][3], col_loads[1], *o_loads):
        x.start()

    def more_rows():
        for x in row_loads[1]:
            x.start()

    hooks = {
        (0, 1): lambda: more_rows(),
        (0, 2): lambda: f_second(0),
        (0, 3): lambda: f_second(1),
        (0, 6): lambda: f_mate(0, (0,)),
        (0, 7): lambda: f_across(0, (1, 3)),
        (1, 0): lambda: f_mate(1, (0,)),
        (1, 1): lambda: f_across(1, (1, 3)),
        (1, 2): lambda: (f_across(0, (2,)), w_second(range(WS))),
        (1, 4): lambda: f_mate(0, (1, 3)),
        (1, 5): lambda: (f_mate(0, (2,)), f_across(1, (2,))),
        (1, 7): lambda: f_mate(1, (1, 3)),
    }
    for m in range(2):
        turn_cols(m)
        for n in range(8):
            gradient(m, n)
            if (m, n) in hooks:
                hooks[m, n]()
    f_done(0)
    project(0, 0)
    f_mate(1, (2,))
    project(0, 1)
    scatter(0, 0)
    scatter(0, 1)
    f_done(1)
    project(1, 0)
    project(1, 1)
    scatter(1, 0)
    scatter(1, 1)
    w_have(range(WS))
    w_mate((0, 1, 3))
    gram_of(0)
    moments(0, 0)
    moments(0, 1)
    gram_of(1)
    moments(1, 0)
    moments(1, 1)
    w_third(range(WS))
    spread(0, 0)
    spread(0, 1)
    spread(1, 0)
    spread(1, 1)
    squares(0)
    squares(1)
    w_mate((2,))
    expand(0)
    expand(1)
    total(0)
    total(1)
    wm_in.arrived()
    for i, n in enumerate(out_bytes):
        all_of = tally.at[pl.ds(0, n)]
        pltpu.make_async_remote_copy(
            src_ref=all_of, dst_ref=all_of, send_sem=ssem.at[i], recv_sem=rsem.at[0],
            device_id=mate, device_id_type=MESH,
        ).wait_send()


def finish_kernel(
    ntp,
    new, ss, wg, ex, w_v, w_o,
    step_v, upd_v, fnew_v, snew_v, copy_v, step_o, upd_o, fnew_o, snew_o, copy_o,
    res, w, st, up, sem_w, sem_s, sem_o,
):
    me = lax.axis_index("fs")
    n, B, C = ex.shape[1:]
    n_ch = sem_o.shape[1]
    loads, outs = [], []

    def store(src, dst, sem):
        o = pltpu.make_async_copy(src, dst, sem)
        o.start()
        outs.append(o)

    for m in range(2):
        loads.append(pltpu.make_async_copy((w_v, w_o)[m], w.at[m], sem_w.at[m]))
        loads[m].start()
        for i in range(2):
            store(new.at[m, i], ((fnew_v, snew_v), (fnew_o, snew_o))[m][i], sem_s.at[m, i])
    for m, (step, upd, copy) in enumerate(((step_v, upd_v, copy_v), (step_o, upd_o, copy_o))):
        mean = jnp.sum(ss[m], keepdims=True) / (n * B * C * ntp)
        scale = step_rate / jnp.sqrt(mean + scale_floor)
        for b in range(n_ch):
            at = pl.ds(b * (n // n_ch), n // n_ch)
            res[m, at] = (wg[m, at].astype(F32) - scale * ex[m, at]).astype(BF16)
            store(res.at[m, at], copy.at[at], sem_o.at[m, b])
        loads[m].wait()
        s = scale * ex[m, me]
        st[m] = s
        up[m] = w[m] - s
        store(st.at[m], step, sem_s.at[m, 2])
        store(up.at[m], upd, sem_s.at[m, 3])
    for o in outs:
        o.wait()


def local(
    n, ntp,
    model_input, value_cotan, mixer_cotan, head_output,
    value_weight, value_factor, value_first, value_second,
    output_weight, output_factor, output_first, output_second,
):
    T, D = model_input.shape
    C = value_cotan.shape[1]
    B, R = value_factor.shape
    k = value_first.shape[0]
    np_ = NZ * NZ
    vm = pl.BlockSpec(memory_space=pltpu.VMEM)
    hbm = pl.BlockSpec(memory_space=pl.ANY)
    mom = jax.ShapeDtypeStruct((k, C), F32)
    wide = jax.ShapeDtypeStruct((B, C), F32)
    full = jax.ShapeDtypeStruct((n, B, C), BF16)
    dma = pltpu.SemaphoreType.DMA
    fg_shape = (2, NZ, NZ, NC, NQ, B // NQ, R)
    new, ss, wg, ex = pl.pallas_call(
        functools.partial(gather_kernel, ntp),
        out_shape=(
            pltpu.VMEM((2, 2, k, C), F32),
            pltpu.VMEM((2, 8, 128), F32),
            pltpu.VMEM((2, NZ, NZ, NC, WS, B // WS, C), BF16),
            pltpu.VMEM((2, n, B, C), F32),
        ),
        in_specs=[hbm] * 12,
        out_specs=(vm,) * 4,
        scratch_shapes=[
            pltpu.VMEM((2, T, D), BF16),
            pltpu.VMEM((2, T, C), BF16),
            pltpu.VMEM((2, C, T), BF16),
            pltpu.VMEM((2, C, D), BF16),
            pltpu.VMEM(fg_shape, BF16),
            pltpu.VMEM((2, NH, np_, NC, k, C // NH), F32),
            pltpu.VMEM((2, NH, np_, k, C // NH), BF16),
            pltpu.VMEM((2, NH, np_, k, C // NH), BF16),
            pltpu.VMEM((2, NH, np_, k, C // NH), BF16),
            pltpu.VMEM((2, NH, np_ - 1, k, C // NH), BF16),
            pltpu.VMEM((2, NH, k, C // NH), F32),
            pltpu.VMEM((2, NH, np_, NC, k, C // NH), BF16),
            pltpu.VMEM((2, 2, R, R), BF16),
            pltpu.VMEM((2, 8, 128), F32),
            pltpu.VMEM((2, ntp, 8, 128), F32),
            pltpu.VMEM((512, 16, 128), BF16),
            pltpu.VMEM((2, B, C), F32),
            pltpu.VMEM((2, 2, k, C), F32),
            dma((2, 4)), dma((2,)), dma((8,)), dma((N_SEMS,)), dma((N_SEMS,)),
        ],
        compiler_params=pltpu.CompilerParams(
            collective_id=0, has_side_effects=True, vmem_limit_bytes=50_000_000
        ),
        name="gather",
    )(
        model_input, value_cotan, mixer_cotan, head_output,
        value_factor.reshape(NQ, B // NQ, R), output_factor.reshape(NQ, B // NQ, R), value_weight, output_weight,
        value_first, output_first, value_second, output_second,
    )
    n_ch = 4
    outs = pl.pallas_call(
        functools.partial(finish_kernel, ntp),
        out_shape=(wide, wide, mom, mom, full) * 2,
        in_specs=[vm] * 4 + [hbm] * 2,
        out_specs=(hbm,) * 10,
        scratch_shapes=[
            pltpu.VMEM((2, n, B, C), BF16),
            pltpu.VMEM((2, B, C), F32),
            pltpu.VMEM((2, B, C), F32),
            pltpu.VMEM((2, B, C), F32),
            dma((2,)), dma((2, 4)), dma((2, n_ch)),
        ],
        compiler_params=pltpu.CompilerParams(vmem_limit_bytes=20_000_000),
        name="finish",
    )(new, ss, wg.reshape(2, n, B, C), ex, value_weight, output_weight)
    return tuple(o.reshape(D, C) if o.ndim == 3 else o for o in outs)


def solution(mesh):
    rows, both, full = P("fs", None), P("fs", "tp"), P(None, "tp")
    return jax.shard_map(
        functools.partial(local, mesh.shape["fs"], mesh.shape["tp"]),
        mesh=mesh,
        in_specs=(rows, both, rows, both) + (both, rows, both, both) * 2,
        out_specs=(both, both, both, both, full) * 2,
        check_vma=False,
    )
```

```python
import functools
import math

import jax
import jax.numpy as jnp
from jax import lax
from jax.experimental import pallas as pl
from jax.experimental.pallas import tpu as pltpu
from jax.sharding import PartitionSpec as P

beta_first = 0.8
beta_second = 0.9
step_rate = 0.02
scale_floor = 0.25
tiny_eps = 1e-08

MESH = pl.DeviceIdType.MESH
F32 = jnp.float32
BF16 = jnp.bfloat16
NZ = 4
NC = 2
NQ = 4
WS = 4
NH = 2
N_SEND, N_RECV = 6, 36
OFFSETS = sorted(
    [(a, b) for a in range(NZ) for b in range(NZ) if a or b],
    key=lambda o: -(min(o[0], NZ - o[0]) + min(o[1], NZ - o[1])),
)


def gather_kernel(
    ntp,
    rows_v, cols_v, rows_o, cols_o,
    fac_v, fac_o, w_v, w_o, first_v, first_o, second_v, second_o,
    new, sst, wg, ex,
    rows, cols, cols_t, grad, fg, pf, send_a, recv_a, send_b, recv_b, mdir,
    dirg, gram, ss, ssg, tally, wide, old,
    sem_rows, sem_cols, sem_in, ssem, rsem,
):
    me = lax.axis_index("fs")
    tp = lax.axis_index("tp")
    z, y, c = me // (NZ * NC), lax.rem(me // NC, NZ), lax.rem(me, NC)
    co = 1 - c
    chip = z * NZ + y
    h = lax.rem(tp, 2)
    T, D = rows_v.shape
    C = cols_v.shape[1]
    QR, R = fac_v.shape[1:]
    WR = w_v.shape[0] // WS

    def up(a, d):
        return lax.rem(a + d, NZ)

    def dn(a, d):
        return lax.rem(a + NZ - d, NZ)

    def plane(zz, yy):
        return ((zz * NZ + yy) * NC + c, tp)

    def across(zz, yy):
        return ((zz * NZ + yy) * NC + co, tp)

    mate = (me - c + co, tp)

    def along_x(d, core=c):
        return (me - c + core, lax.rem(tp + ntp + d, ntp))

    row_bytes = 2 * tally.shape[1] * tally.shape[2]
    n_recv = [0]
    out_bytes = [0]

    def size(ref):
        return math.prod(ref.shape) * jnp.dtype(ref.dtype).itemsize // row_bytes

    class Group:
        def __init__(self):
            self.i, self.rows = n_recv[0], 0
            n_recv[0] += 1

        def arrived(self):
            all_of = tally.at[pl.ds(0, self.rows)]
            pltpu.make_async_remote_copy(
                src_ref=all_of, dst_ref=all_of, send_sem=ssem.at[0], recv_sem=rsem.at[self.i],
                device_id=mate, device_id_type=MESH,
            ).wait_recv()

    class Send:
        def __init__(self, src, dst, group, dev):
            if out_bytes[-1] + size(src) > tally.shape[0]:
                out_bytes.append(0)
            out_bytes[-1] += size(src)
            group.rows += size(src)
            self.copy = pltpu.make_async_remote_copy(
                src_ref=src, dst_ref=dst, send_sem=ssem.at[len(out_bytes) - 1], recv_sem=rsem.at[group.i],
                device_id=dev, device_id_type=MESH,
            )

        def start(self):
            self.copy.start()

    barrier = pltpu.get_barrier_semaphore()
    for dz, dy in OFFSETS:
        pl.semaphore_signal(barrier, inc=1, device_id=across(up(z, dz), up(y, dy)), device_id_type=MESH)
        if dz == 0 or dy == 0:
            pl.semaphore_signal(barrier, inc=1, device_id=plane(up(z, dz), up(y, dy)), device_id_type=MESH)
    pl.semaphore_signal(barrier, inc=1, device_id=mate, device_id_type=MESH)
    for q in range(1, ntp):
        pl.semaphore_signal(barrier, inc=1, device_id=along_x(q, co), device_id_type=MESH)
    for q in (1, -1):
        pl.semaphore_signal(barrier, inc=1, device_id=along_x(q), device_id_type=MESH)

    half = D // 4
    f_loads, w_loads, o_loads, row_loads, col_loads = [], [], [], [[], []], []
    for m, (r, cc, f, w, a, b) in enumerate((
        (rows_v, cols_v, fac_v, w_v, first_v, second_v), (rows_o, cols_o, fac_o, w_o, first_o, second_o)
    )):
        mine = pl.ds(2 * h, 2)
        f_loads.append(pltpu.make_async_copy(f.at[mine], fg.at[m, z, y, c, mine], sem_in.at[m]))
        w_loads.append(pltpu.make_async_copy(w, wide.at[m], sem_in.at[2 + m]))
        o_loads.append(pltpu.make_async_copy(a, old.at[m, 0], sem_in.at[4 + m]))
        o_loads.append(pltpu.make_async_copy(b, old.at[m, 1], sem_in.at[6 + m]))
        col_loads.append(pltpu.make_async_copy(cc, cols.at[m], sem_cols.at[m]))
        for j in range(4):
            at = pl.ds(j * half, half)
            row_loads[m].append(pltpu.make_async_copy(r.at[:, at], rows.at[m, :, at], sem_rows.at[m, j]))
    for x in (*f_loads, *w_loads, col_loads[0], row_loads[0][0], row_loads[0][1]):
        x.start()

    def line(buf, m, s, g, cc, k):
        return buf.at[m, :, dn(y, g), cc, k] if s == 0 else buf.at[m, dn(z, g), :, cc, k]

    def own(buf, m, s, d, k):
        return buf.at[m, dn(z, d), y, c, k] if s == 0 else buf.at[m, z, dn(y, d), c, k]

    def first_dev(s, d):
        return plane(up(z, d), y) if s == 0 else plane(z, up(y, d))

    def second_dev(s, d, to=plane):
        return to(z, up(y, d)) if s == 0 else to(up(z, d), y)

    f1, f2, fx, fm, fxm = {}, {}, {}, {}, {}
    f1_in, f2_in, fx_in, fm_in = {}, {}, {}, {}
    for m in range(2):
        f1_in[m], fm_in[m] = Group(), Group()
        f2_in[m, 1] = f2_in[m, 3] = Group()
        f2_in[m, 2] = Group()
        fx_in[m, 0], fx_in[m, 2] = Group(), Group()
        fx_in[m, 1] = fx_in[m, 3] = Group()
        for s in range(2):
            k, kx = 2 * h + s, 2 * (1 - h) + s
            for d in (2, 1, 3):
                f1[m, s, d] = Send(own(fg, m, s, 0, k), own(fg, m, s, 0, k), f1_in[m], first_dev(s, d))
                f2[m, s, d] = Send(line(fg, m, s, 0, c, k), line(fg, m, s, 0, c, k), f2_in[m, d], second_dev(s, d, across))
            for g in range(NZ):
                held = co if g else c
                a, b = line(fg, m, s, g, held, k), line(fg, m, s, g, held, kx)
                if g == 2:
                    o = line(fg, m, s, 0, c, kx)
                    fx[m, s, g] = Send(o, o, fx_in[m, g], second_dev(s, 2, across))
                else:
                    fx[m, s, g] = Send(a, a, fx_in[m, g], along_x(1 if s == 0 else -1))
                fm[m, s, g] = Send(a, a, fm_in[m], mate)
                fxm[m, s, g] = Send(b, b, fm_in[m], mate)

    def f_first(m):
        for d in (2, 1, 3):
            for s in range(2):
                f1[m, s, d].start()

    def f_second(m):
        f1_in[m].arrived()
        for d in (1, 3, 2):
            for s in range(2):
                f2[m, s, d].start()
        for s in range(2):
            fx[m, s, 0].start()
            fm[m, s, 0].start()

    def f_across(m, gs):
        f2_in[m, gs[0]].arrived()
        for g in gs:
            for s in range(2):
                if g != 2:
                    fx[m, s, g].start()
                fm[m, s, g].start()

    def f_mate(m, gs):
        fx_in[m, gs[0]].arrived()
        for g in gs:
            for s in range(2):
                if g == 0:
                    fx[m, s, 2].start()
                fxm[m, s, g].start()

    def f_done(m):
        fm_in[m].arrived()

    w1, w2, w3, wm = {}, {}, {}, {}

    def part(m, j, g, b):
        two = pl.ds(2 * b, 2)
        return wg.at[m, two, dn(y, g), c, j] if m == 0 else wg.at[m, dn(z, g), two, c, j]

    w1_in, w3_in, wm_in = Group(), Group(), Group()
    w2_in = Group()
    for j in range(WS):
        for m in range(2):
            for d in (2, 1, 3):
                w1[m, j, d] = Send(own(wg, m, m, 0, j), own(wg, m, m, 0, j), w1_in, first_dev(m, d))
            for d in (1, 3):
                w2[m, j, d] = Send(line(wg, m, m, 0, c, j), line(wg, m, m, 0, c, j), w2_in, second_dev(m, d))
                b = d // 2
                w3[m, j, d] = Send(part(m, j, d, b), part(m, j, d, b), w3_in, second_dev(m, d))
    for m in range(2):
        for g in range(NZ):
            a = wg.at[m, :, dn(y, g), c] if m == 0 else wg.at[m, dn(z, g), :, c]
            wm[m, g] = Send(a, a, wm_in, mate)

    def w_own():
        for m in range(2):
            w_loads[m].wait()
            wg[m, z, y, c] = wide[m].reshape(WS, WR, C).astype(BF16)

    def w_first():
        for j in range(WS):
            for d in (2, 1, 3):
                for m in range(2):
                    w1[m, j, d].start()

    def w_second():
        w1_in.arrived()
        for j in range(WS):
            for d in (1, 3):
                for m in range(2):
                    w2[m, j, d].start()

    def w_have():
        w2_in.arrived()

    def w_third():
        for j in range(WS):
            for d in (1, 3):
                for m in range(2):
                    w3[m, j, d].start()

    def w_mate(gs):
        if gs[0] == 2:
            w3_in.arrived()
        for g in gs:
            for m in range(2):
                wm[m, g].start()

    def w_done():
        wm_in.arrived()

    def turn_cols(m):
        col_loads[m].wait()
        for t in range(4):
            at = pl.ds(t * (T // 4), T // 4)
            cols_t[m, :, at] = cols[m, at, :].T

    def gradient(m, n):
        j, b = n // 2, n % 2
        if b == 0:
            row_loads[m][j].wait()
        at, up_to = pl.ds(j * half, half), pl.ds(b * (C // 2), C // 2)
        grad[m, up_to, at] = jnp.dot(cols_t[m, up_to], rows[m, :, at], preferred_element_type=F32).astype(BF16)

    def factor_of(m):
        return fg[m].reshape(D, R)

    CW = C // NH
    sa, sb, sa_in, sb_in = {}, {}, {}, {}
    dp, dp_in, dm, dm_in = {}, {}, {}, {}
    for m in range(2):
        for b in range(NH):
            p = m, b
            sa_in[p], sb_in[p], dp_in[p], dm_in[p] = Group(), Group(), Group(), Group()
            sa[p] = Send(send_a.at[m, b], recv_a.at[m, b], sa_in[p], mate)
            mine = mdir.at[m, b]
            for i, (dz, dy) in enumerate(OFFSETS):
                to = up(z, dz) * NZ + up(y, dy)
                dev = across(up(z, dz), up(y, dy))
                sb[m, b, i] = Send(send_b.at[m, b, to], recv_b.at[m, b, i], sb_in[p], dev)
                dp[m, b, i] = Send(mine, dirg.at[m, b, chip, c], dp_in[p], dev)
            i = len(OFFSETS)
            sb[m, b, i] = Send(send_b.at[m, b, chip], recv_b.at[m, b, i], sb_in[p], mate)
            dp[m, b, i] = Send(mine, dirg.at[m, b, chip, c], dp_in[p], mate)
            dm[p] = Send(dirg.at[m, b, :, co], dirg.at[m, b, :, co], dm_in[p], mate)

    def project(m, b):
        pt = jnp.dot(grad[m, pl.ds(b * CW, CW)], factor_of(m), preferred_element_type=F32)
        pf[m, b] = pt.T.reshape(NZ * NZ, NC, QR, CW)
        send_a[m, b] = pf[m, b, :, c].astype(BF16)
        sa[m, b].start()

    def scatter(m, b):
        sa_in[m, b].arrived()
        send_b[m, b] = (pf[m, b, :, co] + recv_a[m, b].astype(F32)).astype(BF16)
        for i in range(len(OFFSETS) + 1):
            sb[m, b, i].start()

    def moments(m, b):
        at = pl.ds(b * CW, CW)
        if b == 0:
            o_loads[2 * m].wait()
            o_loads[2 * m + 1].wait()
        sb_in[m, b].arrived()
        tot = recv_b[m, b, 0].astype(F32)
        for i in range(1, len(OFFSETS) + 1):
            tot = tot + recv_b[m, b, i].astype(F32)
        f = beta_first * old[m, 0, :, at] + (1.0 - beta_first) * tot
        s = beta_second * old[m, 1, :, at] + (1.0 - beta_second) * tot * tot
        mdir[m, b] = (f / (jnp.sqrt(s) + tiny_eps)).astype(BF16)
        for i in range(len(OFFSETS) + 1):
            dp[m, b, i].start()
        new[m, 0, :, at] = f
        new[m, 1, :, at] = s

    def spread(m, b):
        dp_in[m, b].arrived()
        dm[m, b].start()

    def direction_of(m):
        return jnp.concatenate([dirg[m, b].reshape(R, CW) for b in range(NH)], axis=1)

    def gram_of(m):
        f = factor_of(m)
        ft = f.T
        g = jnp.dot(ft, f, preferred_element_type=F32)
        hi = g.astype(BF16)
        gram[m, 0] = hi
        gram[m, 1] = (g - hi.astype(F32)).astype(BF16)

    sq, sq_in = {}, {}
    for m in range(2):
        sq_in[m] = Group()
        for q in range(1, ntp):
            sq[m, q] = Send(ss.at[m], ssg.at[m, q], sq_in[m], along_x(q, co))

    def squares(m):
        for b in range(NH):
            dm_in[m, b].arrived()
        d = direction_of(m)
        e = jnp.dot(gram[m, 0], d, preferred_element_type=F32)
        e += jnp.dot(gram[m, 1], d, preferred_element_type=F32)
        p = jnp.sum((e * d.astype(F32)).reshape(R // 8, 8, C), axis=0)
        t = p[:, :128]
        for b in range(1, C // 128):
            t = t + p[:, b * 128:(b + 1) * 128]
        ss[m] = t
        for q in range(1, ntp):
            sq[m, q].start()

    def expand(m, bs):
        d = direction_of(m)
        f = fg.at[m]
        for b in bs:
            ex[m, pl.ds(b * NZ * NC, NZ * NC)] = jnp.dot(
                f[b].reshape(D // NZ, R), d, preferred_element_type=F32
            ).reshape(NZ * NC, NQ * QR, C)

    def total(m):
        t = ss[m]
        sq_in[m].arrived()
        for q in range(1, ntp):
            t = t + ssg[m, q]
        sst[m] = t

    assert (len(out_bytes), n_recv[0]) == (N_SEND, N_RECV)

    for x in f_loads:
        x.wait()
    pl.semaphore_wait(barrier, len(OFFSETS) + 2 * (NZ - 1) + 1 + (ntp - 1) + 2)
    f_first(0)
    f_first(1)
    w_own()
    w_first()
    for x in (row_loads[0][2], row_loads[0][3], col_loads[1], *o_loads):
        x.start()

    def more_rows():
        for x in row_loads[1]:
            x.start()

    hooks = {
        (0, 1): lambda: more_rows(),
        (0, 2): lambda: f_second(0),
        (0, 3): lambda: f_second(1),
        (0, 6): lambda: f_mate(0, (0,)),
        (0, 7): lambda: f_across(0, (1, 3)),
        (1, 0): lambda: f_mate(1, (0,)),
        (1, 1): lambda: f_across(1, (1, 3)),
        (1, 2): lambda: (f_across(0, (2,)), w_second()),
        (1, 4): lambda: f_mate(0, (1, 3)),
        (1, 5): lambda: (f_mate(0, (2,)), f_across(1, (2,))),
        (1, 7): lambda: f_mate(1, (1, 3)),
    }
    for m in range(2):
        turn_cols(m)
        for n in range(8):
            gradient(m, n)
            if (m, n) in hooks:
                hooks[m, n]()
    f_done(0)
    project(0, 0)
    f_mate(1, (2,))
    project(0, 1)
    scatter(0, 0)
    scatter(0, 1)
    f_done(1)
    project(1, 0)
    project(1, 1)
    scatter(1, 0)
    scatter(1, 1)
    w_have()
    w_mate((0, 1, 3))
    gram_of(0)
    moments(0, 0)
    moments(0, 1)
    gram_of(1)
    moments(1, 0)
    moments(1, 1)
    w_third()
    spread(0, 0)
    spread(0, 1)
    spread(1, 0)
    spread(1, 1)
    squares(0)
    expand(0, (0, 1))
    squares(1)
    w_mate((2,))
    expand(0, (2, 3))
    expand(1, range(NZ))
    total(0)
    total(1)
    w_done()
    for i, n in enumerate(out_bytes):
        all_of = tally.at[pl.ds(0, n)]
        pltpu.make_async_remote_copy(
            src_ref=all_of, dst_ref=all_of, send_sem=ssem.at[i], recv_sem=rsem.at[0],
            device_id=mate, device_id_type=MESH,
        ).wait_send()


def finish_kernel(
    ntp,
    new, ss, wg, ex, w_v, w_o,
    step_v, upd_v, fnew_v, snew_v, copy_v, step_o, upd_o, fnew_o, snew_o, copy_o,
    res, w, st, up, sem_w, sem_s, sem_o,
):
    me = lax.axis_index("fs")
    n, B, C = ex.shape[1:]
    n_ch = sem_o.shape[1]
    loads, outs = [], []

    def store(src, dst, sem):
        o = pltpu.make_async_copy(src, dst, sem)
        o.start()
        outs.append(o)

    for m in range(2):
        loads.append(pltpu.make_async_copy((w_v, w_o)[m], w.at[m], sem_w.at[m]))
        loads[m].start()
        for i in range(2):
            store(new.at[m, i], ((fnew_v, snew_v), (fnew_o, snew_o))[m][i], sem_s.at[m, i])
    per = n // n_ch
    for m, (step, upd, copy) in enumerate(((step_v, upd_v, copy_v), (step_o, upd_o, copy_o))):
        mean = jnp.sum(ss[m], keepdims=True) / (n * B * C * ntp)
        scale = step_rate / jnp.sqrt(mean + scale_floor)

        @pl.loop(0, n_ch)
        def _(b):
            at = pl.ds(pl.multiple_of(b * per, per), per)
            res[m, at] = (wg[m, at].astype(F32) - scale * ex[m, at]).astype(BF16)
            pltpu.make_async_copy(res.at[m, at], copy.at[at], sem_o.at[m, b]).start()

        for b in range(n_ch):
            at = pl.ds(b * per, per)
            outs.append(pltpu.make_async_copy(res.at[m, at], copy.at[at], sem_o.at[m, b]))
        loads[m].wait()
        s = scale * ex[m, me]
        st[m] = s
        up[m] = w[m] - s
        store(st.at[m], step, sem_s.at[m, 2])
        store(up.at[m], upd, sem_s.at[m, 3])
    for o in outs:
        o.wait()


def local(
    n, ntp,
    model_input, value_cotan, mixer_cotan, head_output,
    value_weight, value_factor, value_first, value_second,
    output_weight, output_factor, output_first, output_second,
):
    T, D = model_input.shape
    C = value_cotan.shape[1]
    B, R = value_factor.shape
    k = value_first.shape[0]
    np_ = NZ * NZ
    vm = pl.BlockSpec(memory_space=pltpu.VMEM)
    hbm = pl.BlockSpec(memory_space=pl.ANY)
    mom = jax.ShapeDtypeStruct((k, C), F32)
    wide = jax.ShapeDtypeStruct((B, C), F32)
    full = jax.ShapeDtypeStruct((n, B, C), BF16)
    dma = pltpu.SemaphoreType.DMA
    fg_shape = (2, NZ, NZ, NC, NQ, B // NQ, R)
    new, ss, wg, ex = pl.pallas_call(
        functools.partial(gather_kernel, ntp),
        out_shape=(
            pltpu.VMEM((2, 2, k, C), F32),
            pltpu.VMEM((2, 8, 128), F32),
            pltpu.VMEM((2, NZ, NZ, NC, WS, B // WS, C), BF16),
            pltpu.VMEM((2, n, B, C), F32),
        ),
        in_specs=[hbm] * 12,
        out_specs=(vm,) * 4,
        scratch_shapes=[
            pltpu.VMEM((2, T, D), BF16),
            pltpu.VMEM((2, T, C), BF16),
            pltpu.VMEM((2, C, T), BF16),
            pltpu.VMEM((2, C, D), BF16),
            pltpu.VMEM(fg_shape, BF16),
            pltpu.VMEM((2, NH, np_, NC, k, C // NH), F32),
            pltpu.VMEM((2, NH, np_, k, C // NH), BF16),
            pltpu.VMEM((2, NH, np_, k, C // NH), BF16),
            pltpu.VMEM((2, NH, np_, k, C // NH), BF16),
            pltpu.VMEM((2, NH, np_, k, C // NH), BF16),
            pltpu.VMEM((2, NH, k, C // NH), BF16),
            pltpu.VMEM((2, NH, np_, NC, k, C // NH), BF16),
            pltpu.VMEM((2, 2, R, R), BF16),
            pltpu.VMEM((2, 8, 128), F32),
            pltpu.VMEM((2, ntp, 8, 128), F32),
            pltpu.VMEM((512, 16, 128), BF16),
            pltpu.VMEM((2, B, C), F32),
            pltpu.VMEM((2, 2, k, C), F32),
            dma((2, 4)), dma((2,)), dma((8,)), dma((N_SEND,)), dma((N_RECV,)),
        ],
        compiler_params=pltpu.CompilerParams(
            collective_id=0, has_side_effects=True, vmem_limit_bytes=50_000_000
        ),
        name="gather",
    )(
        model_input, value_cotan, mixer_cotan, head_output,
        value_factor.reshape(NQ, B // NQ, R), output_factor.reshape(NQ, B // NQ, R), value_weight, output_weight,
        value_first, output_first, value_second, output_second,
    )
    n_ch = 4
    outs = pl.pallas_call(
        functools.partial(finish_kernel, ntp),
        out_shape=(wide, wide, mom, mom, full) * 2,
        in_specs=[vm] * 4 + [hbm] * 2,
        out_specs=(hbm,) * 10,
        scratch_shapes=[
            pltpu.VMEM((2, n, B, C), BF16),
            pltpu.VMEM((2, B, C), F32),
            pltpu.VMEM((2, B, C), F32),
            pltpu.VMEM((2, B, C), F32),
            dma((2,)), dma((2, 4)), dma((2, n_ch)),
        ],
        compiler_params=pltpu.CompilerParams(vmem_limit_bytes=20_000_000),
        name="finish",
    )(new, ss, wg.reshape(2, n, B, C), ex, value_weight, output_weight)
    return tuple(o.reshape(D, C) if o.ndim == 3 else o for o in outs)


def solution(mesh):
    rows, both, full = P("fs", None), P("fs", "tp"), P(None, "tp")
    return jax.shard_map(
        functools.partial(local, mesh.shape["fs"], mesh.shape["tp"]),
        mesh=mesh,
        in_specs=(rows, both, rows, both) + (both, rows, both, both) * 2,
        out_specs=(both, both, both, both, full) * 2,
        check_vma=False,
    )
```

```python
import functools
import math

import jax
import jax.numpy as jnp
from jax import lax
from jax.experimental import pallas as pl
from jax.experimental.pallas import tpu as pltpu
from jax.sharding import PartitionSpec as P

beta_first = 0.8
beta_second = 0.9
step_rate = 0.02
scale_floor = 0.25
tiny_eps = 1e-08

MESH = pl.DeviceIdType.MESH
F32 = jnp.float32
BF16 = jnp.bfloat16
NZ = 4
NC = 2
NQ = 4
WS = 4
NH = 2
N_SEND, N_RECV = 6, 36
OFFSETS = sorted(
    [(a, b) for a in range(NZ) for b in range(NZ) if a or b],
    key=lambda o: -(min(o[0], NZ - o[0]) + min(o[1], NZ - o[1])),
)


def gather_kernel(
    ntp,
    rows_v, cols_v, rows_o, cols_o,
    fac_v, fac_o, w_v, w_o, first_v, first_o, second_v, second_o,
    new, sst, wg, ex,
    rows, cols, cols_t, grad, fg, pf, send_a, recv_a, send_b, recv_b, mdir,
    dirg, gram, ss, ssg, tally, wide, old,
    sem_rows, sem_cols, sem_in, ssem, rsem,
):
    me = lax.axis_index("fs")
    tp = lax.axis_index("tp")
    z, y, c = me // (NZ * NC), lax.rem(me // NC, NZ), lax.rem(me, NC)
    co = 1 - c
    chip = z * NZ + y
    h = lax.rem(tp, 2)
    T, D = rows_v.shape
    C = cols_v.shape[1]
    QR, R = fac_v.shape[1:]
    WR = w_v.shape[0] // WS

    def up(a, d):
        return lax.rem(a + d, NZ)

    def dn(a, d):
        return lax.rem(a + NZ - d, NZ)

    def plane(zz, yy):
        return ((zz * NZ + yy) * NC + c, tp)

    def across(zz, yy):
        return ((zz * NZ + yy) * NC + co, tp)

    mate = (me - c + co, tp)

    def along_x(d, core=c):
        return (me - c + core, lax.rem(tp + ntp + d, ntp))

    row_bytes = 2 * tally.shape[1] * tally.shape[2]
    n_recv = [0]
    out_bytes = [0]

    def size(ref):
        return math.prod(ref.shape) * jnp.dtype(ref.dtype).itemsize // row_bytes

    class Group:
        def __init__(self):
            self.i, self.rows = n_recv[0], 0
            n_recv[0] += 1

        def arrived(self):
            all_of = tally.at[pl.ds(0, self.rows)]
            pltpu.make_async_remote_copy(
                src_ref=all_of, dst_ref=all_of, send_sem=ssem.at[0], recv_sem=rsem.at[self.i],
                device_id=mate, device_id_type=MESH,
            ).wait_recv()

    class Send:
        def __init__(self, src, dst, group, dev):
            if out_bytes[-1] + size(src) > tally.shape[0]:
                out_bytes.append(0)
            out_bytes[-1] += size(src)
            group.rows += size(src)
            self.copy = pltpu.make_async_remote_copy(
                src_ref=src, dst_ref=dst, send_sem=ssem.at[len(out_bytes) - 1], recv_sem=rsem.at[group.i],
                device_id=dev, device_id_type=MESH,
            )

        def start(self):
            self.copy.start()

    barrier = pltpu.get_barrier_semaphore()
    for dz, dy in OFFSETS:
        pl.semaphore_signal(barrier, inc=1, device_id=across(up(z, dz), up(y, dy)), device_id_type=MESH)
        if dz == 0 or dy == 0:
            pl.semaphore_signal(barrier, inc=1, device_id=plane(up(z, dz), up(y, dy)), device_id_type=MESH)
    pl.semaphore_signal(barrier, inc=1, device_id=mate, device_id_type=MESH)
    for q in range(1, ntp):
        pl.semaphore_signal(barrier, inc=1, device_id=along_x(q, co), device_id_type=MESH)
    for q in (1, -1):
        pl.semaphore_signal(barrier, inc=1, device_id=along_x(q), device_id_type=MESH)

    half = D // 4
    f_loads, w_loads, o_loads, row_loads, col_loads = [], [], [], [[], []], []
    for m, (r, cc, f, w, a, b) in enumerate((
        (rows_v, cols_v, fac_v, w_v, first_v, second_v), (rows_o, cols_o, fac_o, w_o, first_o, second_o)
    )):
        mine = pl.ds(2 * h, 2)
        f_loads.append(pltpu.make_async_copy(f.at[mine], fg.at[m, z, y, c, mine], sem_in.at[m]))
        w_loads.append(pltpu.make_async_copy(w, wide.at[m], sem_in.at[2 + m]))
        o_loads.append(pltpu.make_async_copy(a, old.at[m, 0], sem_in.at[4 + m]))
        o_loads.append(pltpu.make_async_copy(b, old.at[m, 1], sem_in.at[6 + m]))
        col_loads.append(pltpu.make_async_copy(cc, cols.at[m], sem_cols.at[m]))
        for j in range(4):
            at = pl.ds(j * half, half)
            row_loads[m].append(pltpu.make_async_copy(r.at[:, at], rows.at[m, :, at], sem_rows.at[m, j]))
    for x in (*f_loads, *w_loads, col_loads[0], row_loads[0][0], row_loads[0][1]):
        x.start()

    def line(buf, m, s, g, cc, k):
        return buf.at[m, :, dn(y, g), cc, k] if s == 0 else buf.at[m, dn(z, g), :, cc, k]

    def own(buf, m, s, d, k):
        return buf.at[m, dn(z, d), y, c, k] if s == 0 else buf.at[m, z, dn(y, d), c, k]

    def first_dev(s, d):
        return plane(up(z, d), y) if s == 0 else plane(z, up(y, d))

    def second_dev(s, d, to=plane):
        return to(z, up(y, d)) if s == 0 else to(up(z, d), y)

    f1, f2, fx, fm, fxm = {}, {}, {}, {}, {}
    f1_in, f2_in, fx_in, fm_in = {}, {}, {}, {}
    for m in range(2):
        f1_in[m], fm_in[m] = Group(), Group()
        f2_in[m, 1] = f2_in[m, 3] = Group()
        f2_in[m, 2] = Group()
        fx_in[m, 0], fx_in[m, 2] = Group(), Group()
        fx_in[m, 1] = fx_in[m, 3] = Group()
        for s in range(2):
            k, kx = 2 * h + s, 2 * (1 - h) + s
            for d in (2, 1, 3):
                f1[m, s, d] = Send(own(fg, m, s, 0, k), own(fg, m, s, 0, k), f1_in[m], first_dev(s, d))
                f2[m, s, d] = Send(line(fg, m, s, 0, c, k), line(fg, m, s, 0, c, k), f2_in[m, d], second_dev(s, d, across))
            for g in range(NZ):
                held = co if g else c
                a, b = line(fg, m, s, g, held, k), line(fg, m, s, g, held, kx)
                if g == 2:
                    o = line(fg, m, s, 0, c, kx)
                    fx[m, s, g] = Send(o, o, fx_in[m, g], second_dev(s, 2, across))
                else:
                    fx[m, s, g] = Send(a, a, fx_in[m, g], along_x(1 if s == 0 else -1))
                fm[m, s, g] = Send(a, a, fm_in[m], mate)
                fxm[m, s, g] = Send(b, b, fm_in[m], mate)

    def f_first(m):
        for d in (2, 1, 3):
            for s in range(2):
                f1[m, s, d].start()

    def f_second(m):
        f1_in[m].arrived()
        for d in (1, 3, 2):
            for s in range(2):
                f2[m, s, d].start()
        for s in range(2):
            fx[m, s, 0].start()
            fm[m, s, 0].start()

    def f_across(m, gs):
        f2_in[m, gs[0]].arrived()
        for g in gs:
            for s in range(2):
                if g != 2:
                    fx[m, s, g].start()
                fm[m, s, g].start()

    def f_mate(m, gs):
        fx_in[m, gs[0]].arrived()
        for g in gs:
            for s in range(2):
                if g == 0:
                    fx[m, s, 2].start()
                fxm[m, s, g].start()

    def f_done(m):
        fm_in[m].arrived()

    w1, w2, w3, wm = {}, {}, {}, {}

    def part(m, j, g, b):
        two = pl.ds(2 * b, 2)
        return wg.at[m, two, dn(y, g), c, j] if m == 0 else wg.at[m, dn(z, g), two, c, j]

    w1_in, w3_in, wm_in = Group(), Group(), Group()
    w2_in = Group()
    for j in range(WS):
        for m in range(2):
            for d in (2, 1, 3):
                w1[m, j, d] = Send(own(wg, m, m, 0, j), own(wg, m, m, 0, j), w1_in, first_dev(m, d))
            for d in (1, 3):
                w2[m, j, d] = Send(line(wg, m, m, 0, c, j), line(wg, m, m, 0, c, j), w2_in, second_dev(m, d))
                b = d // 2
                w3[m, j, d] = Send(part(m, j, d, b), part(m, j, d, b), w3_in, second_dev(m, d))
    for m in range(2):
        for g in range(NZ):
            a = wg.at[m, :, dn(y, g), c] if m == 0 else wg.at[m, dn(z, g), :, c]
            wm[m, g] = Send(a, a, wm_in, mate)

    def w_own():
        for m in range(2):
            w_loads[m].wait()
            wg[m, z, y, c] = wide[m].reshape(WS, WR, C).astype(BF16)

    def w_first():
        for j in range(WS):
            for d in (2, 1, 3):
                for m in range(2):
                    w1[m, j, d].start()

    def w_second():
        w1_in.arrived()
        for j in range(WS):
            for d in (1, 3):
                for m in range(2):
                    w2[m, j, d].start()

    def w_have():
        w2_in.arrived()

    def w_third():
        for j in range(WS):
            for d in (1, 3):
                for m in range(2):
                    w3[m, j, d].start()

    def w_mate(gs):
        if gs[0] == 2:
            w3_in.arrived()
        for g in gs:
            for m in range(2):
                wm[m, g].start()

    def w_done():
        wm_in.arrived()

    def turn_cols(m):
        col_loads[m].wait()
        for t in range(4):
            at = pl.ds(t * (T // 4), T // 4)
            cols_t[m, :, at] = cols[m, at, :].T

    def gradient(m, n):
        j, b = n // 2, n % 2
        if b == 0:
            row_loads[m][j].wait()
        at, up_to = pl.ds(j * half, half), pl.ds(b * (C // 2), C // 2)
        grad[m, up_to, at] = jnp.dot(cols_t[m, up_to], rows[m, :, at], preferred_element_type=F32).astype(BF16)

    def factor_of(m):
        return fg[m].reshape(D, R)

    CW = C // NH
    sa, sb, sa_in, sb_in = {}, {}, {}, {}
    dp, dp_in, dm, dm_in = {}, {}, {}, {}
    for m in range(2):
        for b in range(NH):
            p = m, b
            sa_in[p], sb_in[p], dp_in[p], dm_in[p] = Group(), Group(), Group(), Group()
            sa[p] = Send(send_a.at[m, b], recv_a.at[m, b], sa_in[p], mate)
            mine = mdir.at[m, b]
            for i, (dz, dy) in enumerate(OFFSETS):
                to = up(z, dz) * NZ + up(y, dy)
                dev = across(up(z, dz), up(y, dy))
                sb[m, b, i] = Send(send_b.at[m, b, to], recv_b.at[m, b, i], sb_in[p], dev)
                dp[m, b, i] = Send(mine, dirg.at[m, b, chip, c], dp_in[p], dev)
            i = len(OFFSETS)
            sb[m, b, i] = Send(send_b.at[m, b, chip], recv_b.at[m, b, i], sb_in[p], mate)
            dp[m, b, i] = Send(mine, dirg.at[m, b, chip, c], dp_in[p], mate)
            dm[p] = Send(dirg.at[m, b, :, co], dirg.at[m, b, :, co], dm_in[p], mate)

    def project(m, b):
        pt = jnp.dot(grad[m, pl.ds(b * CW, CW)], factor_of(m), preferred_element_type=F32)
        pf[m, b] = pt.T.reshape(NZ * NZ, NC, QR, CW)
        send_a[m, b] = pf[m, b, :, c].astype(BF16)
        sa[m, b].start()

    def scatter(m, b):
        sa_in[m, b].arrived()
        send_b[m, b] = (pf[m, b, :, co] + recv_a[m, b].astype(F32)).astype(BF16)
        for i in range(len(OFFSETS) + 1):
            sb[m, b, i].start()

    def moments(m, b):
        at = pl.ds(b * CW, CW)
        if b == 0:
            o_loads[2 * m].wait()
            o_loads[2 * m + 1].wait()
        sb_in[m, b].arrived()
        tot = recv_b[m, b, 0].astype(F32)
        for i in range(1, len(OFFSETS) + 1):
            tot = tot + recv_b[m, b, i].astype(F32)
        f = beta_first * old[m, 0, :, at] + (1.0 - beta_first) * tot
        s = beta_second * old[m, 1, :, at] + (1.0 - beta_second) * tot * tot
        mdir[m, b] = (f / (jnp.sqrt(s) + tiny_eps)).astype(BF16)
        for i in range(len(OFFSETS) + 1):
            dp[m, b, i].start()
        new[m, 0, :, at] = f
        new[m, 1, :, at] = s

    def spread(m, b):
        dp_in[m, b].arrived()
        dm[m, b].start()

    def direction_of(m):
        return jnp.concatenate([dirg[m, b].reshape(R, CW) for b in range(NH)], axis=1)

    def gram_of(m):
        f = factor_of(m)
        ft = f.T
        g = jnp.dot(ft, f, preferred_element_type=F32)
        hi = g.astype(BF16)
        gram[m, 0] = hi
        gram[m, 1] = (g - hi.astype(F32)).astype(BF16)

    sq, sq_in = {}, {}
    for m in range(2):
        sq_in[m] = Group()
        for q in range(1, ntp):
            sq[m, q] = Send(ss.at[m], ssg.at[m, q], sq_in[m], along_x(q, co))

    def squares(m):
        for b in range(NH):
            dm_in[m, b].arrived()
        d = direction_of(m)
        e = jnp.dot(gram[m, 0], d, preferred_element_type=F32)
        e += jnp.dot(gram[m, 1], d, preferred_element_type=F32)
        p = jnp.sum((e * d.astype(F32)).reshape(R // 8, 8, C), axis=0)
        t = p[:, :128]
        for b in range(1, C // 128):
            t = t + p[:, b * 128:(b + 1) * 128]
        ss[m] = t
        for q in range(1, ntp):
            sq[m, q].start()

    def expand(m, bs):
        d = direction_of(m)
        f = fg.at[m]
        for b in bs:
            ex[m, pl.ds(b * NZ * NC, NZ * NC)] = jnp.dot(
                f[b].reshape(D // NZ, R), d, preferred_element_type=F32
            ).reshape(NZ * NC, NQ * QR, C)

    def total(m):
        t = ss[m]
        sq_in[m].arrived()
        for q in range(1, ntp):
            t = t + ssg[m, q]
        sst[m] = t

    assert (len(out_bytes), n_recv[0]) == (N_SEND, N_RECV)

    for x in f_loads:
        x.wait()
    pl.semaphore_wait(barrier, len(OFFSETS) + 2 * (NZ - 1) + 1 + (ntp - 1) + 2)
    f_first(0)
    f_first(1)
    w_own()
    w_first()
    for x in (row_loads[0][2], row_loads[0][3], col_loads[1], *o_loads):
        x.start()

    def more_rows():
        for x in row_loads[1]:
            x.start()

    hooks = {
        (0, 1): lambda: more_rows(),
        (0, 2): lambda: f_second(0),
        (0, 3): lambda: f_second(1),
        (0, 7): lambda: (f_mate(0, (0,)), f_across(0, (1, 3))),
        (1, 0): lambda: f_mate(1, (0,)),
        (1, 1): lambda: f_across(1, (1, 3)),
        (1, 2): lambda: (f_across(0, (2,)), w_second()),
        (1, 4): lambda: f_across(1, (2,)),
        (1, 5): lambda: (f_mate(0, (1, 3)), f_mate(0, (2,))),
    }
    for m in range(2):
        turn_cols(m)
        for n in range(8):
            gradient(m, n)
            if (m, n) in hooks:
                hooks[m, n]()
    f_done(0)
    project(0, 0)
    f_mate(1, (1, 3))
    f_mate(1, (2,))
    project(0, 1)
    scatter(0, 0)
    f_done(1)
    project(1, 0)
    scatter(0, 1)
    project(1, 1)
    scatter(1, 0)
    scatter(1, 1)
    gram_of(0)
    moments(0, 0)
    moments(0, 1)
    gram_of(1)
    moments(1, 0)
    moments(1, 1)
    w_have()
    w_third()
    w_mate((0, 1, 3))
    spread(0, 0)
    spread(0, 1)
    spread(1, 0)
    spread(1, 1)
    squares(0)
    expand(0, (0, 1))
    squares(1)
    w_mate((2,))
    expand(0, (2, 3))
    expand(1, range(NZ))
    total(0)
    total(1)
    w_done()
    for i, n in enumerate(out_bytes):
        all_of = tally.at[pl.ds(0, n)]
        pltpu.make_async_remote_copy(
            src_ref=all_of, dst_ref=all_of, send_sem=ssem.at[i], recv_sem=rsem.at[0],
            device_id=mate, device_id_type=MESH,
        ).wait_send()


def finish_kernel(
    ntp,
    new, ss, wg, ex, w_v, w_o,
    step_v, upd_v, fnew_v, snew_v, copy_v, step_o, upd_o, fnew_o, snew_o, copy_o,
    res, w, st, up, sem_w, sem_s, sem_o,
):
    me = lax.axis_index("fs")
    n, B, C = ex.shape[1:]
    n_ch = sem_o.shape[1]
    loads, outs = [], []

    def store(src, dst, sem):
        o = pltpu.make_async_copy(src, dst, sem)
        o.start()
        outs.append(o)

    for m in range(2):
        loads.append(pltpu.make_async_copy((w_v, w_o)[m], w.at[m], sem_w.at[m]))
        loads[m].start()
        for i in range(2):
            store(new.at[m, i], ((fnew_v, snew_v), (fnew_o, snew_o))[m][i], sem_s.at[m, i])
    per = n // n_ch
    for m, (step, upd, copy) in enumerate(((step_v, upd_v, copy_v), (step_o, upd_o, copy_o))):
        mean = jnp.sum(ss[m], keepdims=True) / (n * B * C * ntp)
        scale = step_rate / jnp.sqrt(mean + scale_floor)

        @pl.loop(0, n_ch)
        def _(b):
            at = pl.ds(pl.multiple_of(b * per, per), per)
            res[m, at] = (wg[m, at].astype(F32) - scale * ex[m, at]).astype(BF16)
            pltpu.make_async_copy(res.at[m, at], copy.at[at], sem_o.at[m, b]).start()

        for b in range(n_ch):
            at = pl.ds(b * per, per)
            outs.append(pltpu.make_async_copy(res.at[m, at], copy.at[at], sem_o.at[m, b]))
        loads[m].wait()
        s = scale * ex[m, me]
        st[m] = s
        up[m] = w[m] - s
        store(st.at[m], step, sem_s.at[m, 2])
        store(up.at[m], upd, sem_s.at[m, 3])
    for o in outs:
        o.wait()


def local(
    n, ntp,
    model_input, value_cotan, mixer_cotan, head_output,
    value_weight, value_factor, value_first, value_second,
    output_weight, output_factor, output_first, output_second,
):
    T, D = model_input.shape
    C = value_cotan.shape[1]
    B, R = value_factor.shape
    k = value_first.shape[0]
    np_ = NZ * NZ
    vm = pl.BlockSpec(memory_space=pltpu.VMEM)
    hbm = pl.BlockSpec(memory_space=pl.ANY)
    mom = jax.ShapeDtypeStruct((k, C), F32)
    wide = jax.ShapeDtypeStruct((B, C), F32)
    full = jax.ShapeDtypeStruct((n, B, C), BF16)
    dma = pltpu.SemaphoreType.DMA
    fg_shape = (2, NZ, NZ, NC, NQ, B // NQ, R)
    new, ss, wg, ex = pl.pallas_call(
        functools.partial(gather_kernel, ntp),
        out_shape=(
            pltpu.VMEM((2, 2, k, C), F32),
            pltpu.VMEM((2, 8, 128), F32),
            pltpu.VMEM((2, NZ, NZ, NC, WS, B // WS, C), BF16),
            pltpu.VMEM((2, n, B, C), F32),
        ),
        in_specs=[hbm] * 12,
        out_specs=(vm,) * 4,
        scratch_shapes=[
            pltpu.VMEM((2, T, D), BF16),
            pltpu.VMEM((2, T, C), BF16),
            pltpu.VMEM((2, C, T), BF16),
            pltpu.VMEM((2, C, D), BF16),
            pltpu.VMEM(fg_shape, BF16),
            pltpu.VMEM((2, NH, np_, NC, k, C // NH), F32),
            pltpu.VMEM((2, NH, np_, k, C // NH), BF16),
            pltpu.VMEM((2, NH, np_, k, C // NH), BF16),
            pltpu.VMEM((2, NH, np_, k, C // NH), BF16),
            pltpu.VMEM((2, NH, np_, k, C // NH), BF16),
            pltpu.VMEM((2, NH, k, C // NH), BF16),
            pltpu.VMEM((2, NH, np_, NC, k, C // NH), BF16),
            pltpu.VMEM((2, 2, R, R), BF16),
            pltpu.VMEM((2, 8, 128), F32),
            pltpu.VMEM((2, ntp, 8, 128), F32),
            pltpu.VMEM((512, 16, 128), BF16),
            pltpu.VMEM((2, B, C), F32),
            pltpu.VMEM((2, 2, k, C), F32),
            dma((2, 4)), dma((2,)), dma((8,)), dma((N_SEND,)), dma((N_RECV,)),
        ],
        compiler_params=pltpu.CompilerParams(
            collective_id=0, has_side_effects=True, vmem_limit_bytes=50_000_000
        ),
        name="gather",
    )(
        model_input, value_cotan, mixer_cotan, head_output,
        value_factor.reshape(NQ, B // NQ, R), output_factor.reshape(NQ, B // NQ, R), value_weight, output_weight,
        value_first, output_first, value_second, output_second,
    )
    n_ch = 4
    outs = pl.pallas_call(
        functools.partial(finish_kernel, ntp),
        out_shape=(wide, wide, mom, mom, full) * 2,
        in_specs=[vm] * 4 + [hbm] * 2,
        out_specs=(hbm,) * 10,
        scratch_shapes=[
            pltpu.VMEM((2, n, B, C), BF16),
            pltpu.VMEM((2, B, C), F32),
            pltpu.VMEM((2, B, C), F32),
            pltpu.VMEM((2, B, C), F32),
            dma((2,)), dma((2, 4)), dma((2, n_ch)),
        ],
        compiler_params=pltpu.CompilerParams(vmem_limit_bytes=20_000_000),
        name="finish",
    )(new, ss, wg.reshape(2, n, B, C), ex, value_weight, output_weight)
    return tuple(o.reshape(D, C) if o.ndim == 3 else o for o in outs)


def solution(mesh):
    rows, both, full = P("fs", None), P("fs", "tp"), P(None, "tp")
    return jax.shard_map(
        functools.partial(local, mesh.shape["fs"], mesh.shape["tp"]),
        mesh=mesh,
        in_specs=(rows, both, rows, both) + (both, rows, both, both) * 2,
        out_specs=(both, both, both, both, full) * 2,
        check_vma=False,
    )
```

```python
import functools
import math

import jax
import jax.numpy as jnp
from jax import lax
from jax.experimental import pallas as pl
from jax.experimental.pallas import tpu as pltpu
from jax.sharding import PartitionSpec as P

beta_first = 0.8
beta_second = 0.9
step_rate = 0.02
scale_floor = 0.25
tiny_eps = 1e-08

MESH = pl.DeviceIdType.MESH
F32 = jnp.float32
BF16 = jnp.bfloat16
NZ = 4
NC = 2
NQ = 4
WS = 4
NH = 2
N_SEND, N_RECV = 6, 36
OFFSETS = sorted(
    [(a, b) for a in range(NZ) for b in range(NZ) if a or b],
    key=lambda o: -(min(o[0], NZ - o[0]) + min(o[1], NZ - o[1])),
)


def gather_kernel(
    ntp,
    rows_v, cols_v, rows_o, cols_o,
    fac_v, fac_o, w_v, w_o, first_v, first_o, second_v, second_o,
    new, sst, wg, ex,
    rows, cols, cols_t, grad, fg, pf, send_a, recv_a, send_b, recv_b, mdir,
    dirg, gram, ss, ssg, tally, wide, old,
    sem_rows, sem_cols, sem_in, ssem, rsem,
):
    me = lax.axis_index("fs")
    tp = lax.axis_index("tp")
    z, y, c = me // (NZ * NC), lax.rem(me // NC, NZ), lax.rem(me, NC)
    co = 1 - c
    chip = z * NZ + y
    h = lax.rem(tp, 2)
    T, D = rows_v.shape
    C = cols_v.shape[1]
    QR, R = fac_v.shape[1:]
    WR = w_v.shape[0] // WS

    def up(a, d):
        return lax.rem(a + d, NZ)

    def dn(a, d):
        return lax.rem(a + NZ - d, NZ)

    def plane(zz, yy):
        return ((zz * NZ + yy) * NC + c, tp)

    def across(zz, yy):
        return ((zz * NZ + yy) * NC + co, tp)

    mate = (me - c + co, tp)

    def along_x(d, core=c):
        return (me - c + core, lax.rem(tp + ntp + d, ntp))

    row_bytes = 2 * tally.shape[1] * tally.shape[2]
    n_recv = [0]
    out_bytes = [0]

    def size(ref):
        return math.prod(ref.shape) * jnp.dtype(ref.dtype).itemsize // row_bytes

    class Group:
        def __init__(self):
            self.i, self.rows = n_recv[0], 0
            n_recv[0] += 1

        def arrived(self):
            all_of = tally.at[pl.ds(0, self.rows)]
            pltpu.make_async_remote_copy(
                src_ref=all_of, dst_ref=all_of, send_sem=ssem.at[0], recv_sem=rsem.at[self.i],
                device_id=mate, device_id_type=MESH,
            ).wait_recv()

    class Send:
        def __init__(self, src, dst, group, dev):
            if out_bytes[-1] + size(src) > tally.shape[0]:
                out_bytes.append(0)
            out_bytes[-1] += size(src)
            group.rows += size(src)
            self.copy = pltpu.make_async_remote_copy(
                src_ref=src, dst_ref=dst, send_sem=ssem.at[len(out_bytes) - 1], recv_sem=rsem.at[group.i],
                device_id=dev, device_id_type=MESH,
            )

        def start(self):
            self.copy.start()

    barrier = pltpu.get_barrier_semaphore()
    for dz, dy in OFFSETS:
        pl.semaphore_signal(barrier, inc=1, device_id=across(up(z, dz), up(y, dy)), device_id_type=MESH)
        if dz == 0 or dy == 0:
            pl.semaphore_signal(barrier, inc=1, device_id=plane(up(z, dz), up(y, dy)), device_id_type=MESH)
    pl.semaphore_signal(barrier, inc=1, device_id=mate, device_id_type=MESH)
    for q in range(1, ntp):
        pl.semaphore_signal(barrier, inc=1, device_id=along_x(q, co), device_id_type=MESH)
    for q in (1, -1):
        pl.semaphore_signal(barrier, inc=1, device_id=along_x(q), device_id_type=MESH)

    half = D // 4
    f_loads, w_loads, o_loads, row_loads, col_loads = [], [], [], [[], []], []
    for m, (r, cc, f, w, a, b) in enumerate((
        (rows_v, cols_v, fac_v, w_v, first_v, second_v), (rows_o, cols_o, fac_o, w_o, first_o, second_o)
    )):
        mine = pl.ds(2 * h, 2)
        f_loads.append(pltpu.make_async_copy(f.at[mine], fg.at[m, z, y, c, mine], sem_in.at[m]))
        w_loads.append(pltpu.make_async_copy(w, wide.at[m], sem_in.at[2 + m]))
        o_loads.append(pltpu.make_async_copy(a, old.at[m, 0], sem_in.at[4 + m]))
        o_loads.append(pltpu.make_async_copy(b, old.at[m, 1], sem_in.at[6 + m]))
        col_loads.append(pltpu.make_async_copy(cc, cols.at[m], sem_cols.at[m]))
        for j in range(4):
            at = pl.ds(j * half, half)
            row_loads[m].append(pltpu.make_async_copy(r.at[:, at], rows.at[m, :, at], sem_rows.at[m, j]))
    for x in (*f_loads, *w_loads, col_loads[0], row_loads[0][0], row_loads[0][1]):
        x.start()

    def line(buf, m, s, g, cc, k):
        return buf.at[m, :, dn(y, g), cc, k] if s == 0 else buf.at[m, dn(z, g), :, cc, k]

    def own(buf, m, s, d, k):
        return buf.at[m, dn(z, d), y, c, k] if s == 0 else buf.at[m, z, dn(y, d), c, k]

    def first_dev(s, d):
        return plane(up(z, d), y) if s == 0 else plane(z, up(y, d))

    def second_dev(s, d, to=plane):
        return to(z, up(y, d)) if s == 0 else to(up(z, d), y)

    f1, f2, fx, fm, fxm = {}, {}, {}, {}, {}
    f1_in, f2_in, fx_in, fm_in = {}, {}, {}, {}
    for m in range(2):
        f1_in[m], fm_in[m] = Group(), Group()
        f2_in[m, 1] = f2_in[m, 3] = Group()
        f2_in[m, 2] = Group()
        fx_in[m, 0], fx_in[m, 2] = Group(), Group()
        fx_in[m, 1] = fx_in[m, 3] = Group()
        for s in range(2):
            k, kx = 2 * h + s, 2 * (1 - h) + s
            for d in (2, 1, 3):
                f1[m, s, d] = Send(own(fg, m, s, 0, k), own(fg, m, s, 0, k), f1_in[m], first_dev(s, d))
                f2[m, s, d] = Send(line(fg, m, s, 0, c, k), line(fg, m, s, 0, c, k), f2_in[m, d], second_dev(s, d, across))
            for g in range(NZ):
                held = co if g else c
                a, b = line(fg, m, s, g, held, k), line(fg, m, s, g, held, kx)
                if g == 2:
                    o = line(fg, m, s, 0, c, kx)
                    fx[m, s, g] = Send(o, o, fx_in[m, g], second_dev(s, 2, across))
                else:
                    fx[m, s, g] = Send(a, a, fx_in[m, g], along_x(1 if s == 0 else -1))
                fm[m, s, g] = Send(a, a, fm_in[m], mate)
                fxm[m, s, g] = Send(b, b, fm_in[m], mate)

    def f_first(m):
        for d in (2, 1, 3):
            for s in range(2):
                f1[m, s, d].start()

    def f_second(m):
        f1_in[m].arrived()
        for d in (1, 3, 2):
            for s in range(2):
                f2[m, s, d].start()
        for s in range(2):
            fx[m, s, 0].start()
            fm[m, s, 0].start()

    def f_across(m, gs):
        f2_in[m, gs[0]].arrived()
        for g in gs:
            for s in range(2):
                if g != 2:
                    fx[m, s, g].start()
                fm[m, s, g].start()

    def f_mate(m, gs):
        fx_in[m, gs[0]].arrived()
        for g in gs:
            for s in range(2):
                if g == 0:
                    fx[m, s, 2].start()
                fxm[m, s, g].start()

    def f_done(m):
        fm_in[m].arrived()

    w1, w2, w3, wm = {}, {}, {}, {}

    def part(m, j, g, b):
        two = pl.ds(2 * b, 2)
        return wg.at[m, two, dn(y, g), c, j] if m == 0 else wg.at[m, dn(z, g), two, c, j]

    w1_in, w3_in, wm_in = Group(), Group(), Group()
    w2_in = Group()
    for j in range(WS):
        for m in range(2):
            for d in (2, 1, 3):
                w1[m, j, d] = Send(own(wg, m, m, 0, j), own(wg, m, m, 0, j), w1_in, first_dev(m, d))
            for d in (1, 3):
                w2[m, j, d] = Send(line(wg, m, m, 0, c, j), line(wg, m, m, 0, c, j), w2_in, second_dev(m, d))
                b = d // 2
                w3[m, j, d] = Send(part(m, j, d, b), part(m, j, d, b), w3_in, second_dev(m, d))
    for m in range(2):
        for g in range(NZ):
            a = wg.at[m, :, dn(y, g), c] if m == 0 else wg.at[m, dn(z, g), :, c]
            wm[m, g] = Send(a, a, wm_in, mate)

    def w_own():
        for m in range(2):
            w_loads[m].wait()
            wg[m, z, y, c] = wide[m].reshape(WS, WR, C).astype(BF16)

    def w_first():
        for j in range(WS):
            for d in (2, 1, 3):
                for m in range(2):
                    w1[m, j, d].start()

    def w_second():
        w1_in.arrived()
        for j in range(WS):
            for d in (1, 3):
                for m in range(2):
                    w2[m, j, d].start()

    def w_have():
        w2_in.arrived()

    def w_third():
        for j in range(WS):
            for d in (1, 3):
                for m in range(2):
                    w3[m, j, d].start()

    def w_mate(gs):
        if gs[0] == 2:
            w3_in.arrived()
        for g in gs:
            for m in range(2):
                wm[m, g].start()

    def w_done():
        wm_in.arrived()

    def turn_cols(m):
        col_loads[m].wait()
        for t in range(4):
            at = pl.ds(t * (T // 4), T // 4)
            cols_t[m, :, at] = cols[m, at, :].T

    def gradient(m, n):
        j, b = n // 2, n % 2
        if b == 0:
            row_loads[m][j].wait()
        at, up_to = pl.ds(j * half, half), pl.ds(b * (C // 2), C // 2)
        grad[m, up_to, at] = jnp.dot(cols_t[m, up_to], rows[m, :, at], preferred_element_type=F32).astype(BF16)

    def factor_of(m):
        return fg[m].reshape(D, R)

    CW = C // NH
    sa, sb, sa_in, sb_in = {}, {}, {}, {}
    dp, dp_in, dm, dm_in = {}, {}, {}, {}
    for m in range(2):
        for b in range(NH):
            p = m, b
            sa_in[p], sb_in[p], dp_in[p], dm_in[p] = Group(), Group(), Group(), Group()
            sa[p] = Send(send_a.at[m, b], recv_a.at[m, b], sa_in[p], mate)
            mine = mdir.at[m, b]
            for i, (dz, dy) in enumerate(OFFSETS):
                to = up(z, dz) * NZ + up(y, dy)
                dev = across(up(z, dz), up(y, dy))
                sb[m, b, i] = Send(send_b.at[m, b, to], recv_b.at[m, b, i], sb_in[p], dev)
                dp[m, b, i] = Send(mine, dirg.at[m, b, chip, c], dp_in[p], dev)
            i = len(OFFSETS)
            sb[m, b, i] = Send(send_b.at[m, b, chip], recv_b.at[m, b, i], sb_in[p], mate)
            dp[m, b, i] = Send(mine, dirg.at[m, b, chip, c], dp_in[p], mate)
            dm[p] = Send(dirg.at[m, b, :, co], dirg.at[m, b, :, co], dm_in[p], mate)

    def project(m, b):
        pt = jnp.dot(grad[m, pl.ds(b * CW, CW)], factor_of(m), preferred_element_type=F32)
        pf[m, b] = pt.T.reshape(NZ * NZ, NC, QR, CW)
        send_a[m, b] = pf[m, b, :, c].astype(BF16)
        sa[m, b].start()

    def scatter(m, b):
        sa_in[m, b].arrived()
        send_b[m, b] = (pf[m, b, :, co] + recv_a[m, b].astype(F32)).astype(BF16)
        for i in range(len(OFFSETS) + 1):
            sb[m, b, i].start()

    def moments(m, b):
        at = pl.ds(b * CW, CW)
        if b == 0:
            o_loads[2 * m].wait()
            o_loads[2 * m + 1].wait()
        sb_in[m, b].arrived()
        tot = recv_b[m, b, 0].astype(F32)
        for i in range(1, len(OFFSETS) + 1):
            tot = tot + recv_b[m, b, i].astype(F32)
        f = beta_first * old[m, 0, :, at] + (1.0 - beta_first) * tot
        s = beta_second * old[m, 1, :, at] + (1.0 - beta_second) * tot * tot
        mdir[m, b] = (f / (jnp.sqrt(s) + tiny_eps)).astype(BF16)
        for i in range(len(OFFSETS) + 1):
            dp[m, b, i].start()
        new[m, 0, :, at] = f
        new[m, 1, :, at] = s

    def spread(m, b):
        dp_in[m, b].arrived()
        dm[m, b].start()

    def direction_of(m):
        return jnp.concatenate([dirg[m, b].reshape(R, CW) for b in range(NH)], axis=1)

    def gram_of(m):
        f = factor_of(m)
        ft = f.T
        g = jnp.dot(ft, f, preferred_element_type=F32)
        hi = g.astype(BF16)
        gram[m, 0] = hi
        gram[m, 1] = (g - hi.astype(F32)).astype(BF16)

    sq, sq_in = {}, {}
    for m in range(2):
        sq_in[m] = Group()
        for q in range(1, ntp):
            sq[m, q] = Send(ss.at[m], ssg.at[m, q], sq_in[m], along_x(q, co))

    def squares(m):
        for b in range(NH):
            dm_in[m, b].arrived()
        d = direction_of(m)
        e = jnp.dot(gram[m, 0], d, preferred_element_type=F32)
        e += jnp.dot(gram[m, 1], d, preferred_element_type=F32)
        p = jnp.sum((e * d.astype(F32)).reshape(R // 8, 8, C), axis=0)
        t = p[:, :128]
        for b in range(1, C // 128):
            t = t + p[:, b * 128:(b + 1) * 128]
        ss[m] = t
        for q in range(1, ntp):
            sq[m, q].start()

    def expand(m, bs):
        d = direction_of(m)
        f = fg.at[m]
        for b in bs:
            ex[m, pl.ds(b * NZ * NC, NZ * NC)] = jnp.dot(
                f[b].reshape(D // NZ, R), d, preferred_element_type=F32
            ).reshape(NZ * NC, NQ * QR, C)

    def total(m):
        t = ss[m]
        sq_in[m].arrived()
        for q in range(1, ntp):
            t = t + ssg[m, q]
        sst[m] = t

    assert (len(out_bytes), n_recv[0]) == (N_SEND, N_RECV)

    for x in f_loads:
        x.wait()
    pl.semaphore_wait(barrier, len(OFFSETS) + 2 * (NZ - 1) + 1 + (ntp - 1) + 2)
    f_first(0)
    f_first(1)
    w_own()
    w_first()
    for x in (row_loads[0][2], row_loads[0][3], col_loads[1], *o_loads):
        x.start()

    def more_rows():
        for x in row_loads[1]:
            x.start()

    hooks = {
        (0, 1): lambda: more_rows(),
        (0, 2): lambda: f_second(0),
        (0, 3): lambda: f_second(1),
        (0, 7): lambda: (f_mate(0, (0,)), f_across(0, (1, 3))),
        (1, 0): lambda: f_mate(1, (0,)),
        (1, 1): lambda: f_across(1, (1, 3)),
        (1, 2): lambda: (f_across(0, (2,)), w_second()),
        (1, 4): lambda: f_across(1, (2,)),
        (1, 5): lambda: (f_mate(0, (1, 3)), f_mate(0, (2,))),
    }
    for m in range(2):
        turn_cols(m)
        for n in range(8):
            gradient(m, n)
            if (m, n) in hooks:
                hooks[m, n]()
    f_done(0)
    project(0, 0)
    f_mate(1, (1, 3))
    f_mate(1, (2,))
    project(0, 1)
    scatter(0, 0)
    f_done(1)
    project(1, 0)
    scatter(0, 1)
    project(1, 1)
    scatter(1, 0)
    scatter(1, 1)
    gram_of(0)
    moments(0, 0)
    moments(0, 1)
    gram_of(1)
    moments(1, 0)
    moments(1, 1)
    w_have()
    w_third()
    w_mate((0, 1, 3))
    spread(0, 0)
    spread(0, 1)
    spread(1, 0)
    squares(0)
    spread(1, 1)
    expand(0, (0, 1, 2))
    squares(1)
    w_mate((2,))
    expand(0, (3,))
    expand(1, range(NZ))
    total(0)
    total(1)
    w_done()
    for i, n in enumerate(out_bytes):
        all_of = tally.at[pl.ds(0, n)]
        pltpu.make_async_remote_copy(
            src_ref=all_of, dst_ref=all_of, send_sem=ssem.at[i], recv_sem=rsem.at[0],
            device_id=mate, device_id_type=MESH,
        ).wait_send()


def finish_kernel(
    ntp,
    new, ss, wg, ex, w_v, w_o,
    step_v, upd_v, fnew_v, snew_v, copy_v, step_o, upd_o, fnew_o, snew_o, copy_o,
    res, w, st, up, sem_w, sem_s, sem_o,
):
    me = lax.axis_index("fs")
    n, B, C = ex.shape[1:]
    n_ch = sem_o.shape[1]
    loads, outs = [], []

    def store(src, dst, sem):
        o = pltpu.make_async_copy(src, dst, sem)
        o.start()
        outs.append(o)

    for m in range(2):
        loads.append(pltpu.make_async_copy((w_v, w_o)[m], w.at[m], sem_w.at[m]))
        loads[m].start()
        for i in range(2):
            store(new.at[m, i], ((fnew_v, snew_v), (fnew_o, snew_o))[m][i], sem_s.at[m, i])
    per = n // n_ch
    for m, (step, upd, copy) in enumerate(((step_v, upd_v, copy_v), (step_o, upd_o, copy_o))):
        mean = jnp.sum(ss[m], keepdims=True) / (n * B * C * ntp)
        scale = step_rate / jnp.sqrt(mean + scale_floor)

        @pl.loop(0, n_ch)
        def _(b):
            at = pl.ds(pl.multiple_of(b * per, per), per)
            res[m, at] = (wg[m, at].astype(F32) - scale * ex[m, at]).astype(BF16)
            pltpu.make_async_copy(res.at[m, at], copy.at[at], sem_o.at[m, b]).start()

        for b in range(n_ch):
            at = pl.ds(b * per, per)
            outs.append(pltpu.make_async_copy(res.at[m, at], copy.at[at], sem_o.at[m, b]))
        loads[m].wait()
        s = scale * ex[m, me]
        st[m] = s
        up[m] = w[m] - s
        store(st.at[m], step, sem_s.at[m, 2])
        store(up.at[m], upd, sem_s.at[m, 3])
    for o in outs:
        o.wait()


def local(
    n, ntp,
    model_input, value_cotan, mixer_cotan, head_output,
    value_weight, value_factor, value_first, value_second,
    output_weight, output_factor, output_first, output_second,
):
    T, D = model_input.shape
    C = value_cotan.shape[1]
    B, R = value_factor.shape
    k = value_first.shape[0]
    np_ = NZ * NZ
    vm = pl.BlockSpec(memory_space=pltpu.VMEM)
    hbm = pl.BlockSpec(memory_space=pl.ANY)
    mom = jax.ShapeDtypeStruct((k, C), F32)
    wide = jax.ShapeDtypeStruct((B, C), F32)
    full = jax.ShapeDtypeStruct((n, B, C), BF16)
    dma = pltpu.SemaphoreType.DMA
    fg_shape = (2, NZ, NZ, NC, NQ, B // NQ, R)
    new, ss, wg, ex = pl.pallas_call(
        functools.partial(gather_kernel, ntp),
        out_shape=(
            pltpu.VMEM((2, 2, k, C), F32),
            pltpu.VMEM((2, 8, 128), F32),
            pltpu.VMEM((2, NZ, NZ, NC, WS, B // WS, C), BF16),
            pltpu.VMEM((2, n, B, C), F32),
        ),
        in_specs=[hbm] * 12,
        out_specs=(vm,) * 4,
        scratch_shapes=[
            pltpu.VMEM((2, T, D), BF16),
            pltpu.VMEM((2, T, C), BF16),
            pltpu.VMEM((2, C, T), BF16),
            pltpu.VMEM((2, C, D), BF16),
            pltpu.VMEM(fg_shape, BF16),
            pltpu.VMEM((2, NH, np_, NC, k, C // NH), F32),
            pltpu.VMEM((2, NH, np_, k, C // NH), BF16),
            pltpu.VMEM((2, NH, np_, k, C // NH), BF16),
            pltpu.VMEM((2, NH, np_, k, C // NH), BF16),
            pltpu.VMEM((2, NH, np_, k, C // NH), BF16),
            pltpu.VMEM((2, NH, k, C // NH), BF16),
            pltpu.VMEM((2, NH, np_, NC, k, C // NH), BF16),
            pltpu.VMEM((2, 2, R, R), BF16),
            pltpu.VMEM((2, 8, 128), F32),
            pltpu.VMEM((2, ntp, 8, 128), F32),
            pltpu.VMEM((512, 16, 128), BF16),
            pltpu.VMEM((2, B, C), F32),
            pltpu.VMEM((2, 2, k, C), F32),
            dma((2, 4)), dma((2,)), dma((8,)), dma((N_SEND,)), dma((N_RECV,)),
        ],
        compiler_params=pltpu.CompilerParams(
            collective_id=0, has_side_effects=True, vmem_limit_bytes=50_000_000
        ),
        name="gather",
    )(
        model_input, value_cotan, mixer_cotan, head_output,
        value_factor.reshape(NQ, B // NQ, R), output_factor.reshape(NQ, B // NQ, R), value_weight, output_weight,
        value_first, output_first, value_second, output_second,
    )
    n_ch = 4
    outs = pl.pallas_call(
        functools.partial(finish_kernel, ntp),
        out_shape=(wide, wide, mom, mom, full) * 2,
        in_specs=[vm] * 4 + [hbm] * 2,
        out_specs=(hbm,) * 10,
        scratch_shapes=[
            pltpu.VMEM((2, n, B, C), BF16),
            pltpu.VMEM((2, B, C), F32),
            pltpu.VMEM((2, B, C), F32),
            pltpu.VMEM((2, B, C), F32),
            dma((2,)), dma((2, 4)), dma((2, n_ch)),
        ],
        compiler_params=pltpu.CompilerParams(vmem_limit_bytes=20_000_000),
        name="finish",
    )(new, ss, wg.reshape(2, n, B, C), ex, value_weight, output_weight)
    return tuple(o.reshape(D, C) if o.ndim == 3 else o for o in outs)


def solution(mesh):
    rows, both, full = P("fs", None), P("fs", "tp"), P(None, "tp")
    return jax.shard_map(
        functools.partial(local, mesh.shape["fs"], mesh.shape["tp"]),
        mesh=mesh,
        in_specs=(rows, both, rows, both) + (both, rows, both, both) * 2,
        out_specs=(both, both, both, both, full) * 2,
        check_vma=False,
    )
```
